32 devices in a mesh: sp: 8 (over z, x), tp: 4 (over y, core).
Axes of the slice: x: 2, y: 2, z: 4, core: 2. Of those that a mesh axis runs over, the one named last changes fastest.
Arguments:
- outer_gate: bfloat16 [512, 3072], P('tp', 'sp'), may hold values from -6 to 6
- inner_gate: bfloat16 [512, 3072], P('tp', 'sp'), may hold values from -6 to 6
- conv_input: bfloat16 [512, 3072], P('tp', 'sp'), may hold values from -6 to 6
- conv_taps: bfloat16 [3, 512], P(None, 'tp'), may hold values from -3.5 to 3.5
- mix_weight: bfloat16 [512, 2048], P(None, 'tp'), may hold values from -0.25 to 0.25
- residual: bfloat16 [3072, 2048], P('sp', 'tp'), may hold values from -24 to 24
- norm_gain: bfloat16 [2048], P('tp'), may hold values from 0.099609375 to 1.8984375
- routes: int32 [3072, 2], P('sp'), may hold values from 0 to 15, all different within a row; in each aligned block of 384 rows (0 to 383, 384 to 767, ...) at most 96 rows name the same one
- route_scores: float32 [3072, 2], P('sp'), may hold values from 0.05 to 1
- expert_gate: bfloat16 [16, 2048, 2048], P('sp', None, 'tp'), may hold values from -0.125 to 0.125
- expert_up: bfloat16 [16, 2048, 2048], P('sp', None, 'tp'), may hold values from -0.125 to 0.125
- expert_down: bfloat16 [16, 2048, 2048], P('sp', None, 'tp'), may hold values from -0.125 to 0.125
- shared_gate: bfloat16 [2048, 512], P(None, 'tp'), may hold values from -0.125 to 0.125
- shared_up: bfloat16 [2048, 512], P(None, 'tp'), may hold values from -0.125 to 0.125
- shared_down: bfloat16 [512, 2048], P(None, 'tp'), may hold values from -0.25 to 0.25
Outputs:
- layer_out: bfloat16 [3072, 2048], P('sp', 'tp')
The draws below stay inside these ranges and needn't reach their ends.
Inputs may be any that keep to these rules, and one draw needn't show every extreme that they name: `routes`: within the rows of one index of sp (384 tokens), no expert is named by more than 96 of the token and choice pairs, a bound that some block reaches; the experts of one token differ.
All inputs are finite; a program needn't handle non-finite values.
Results may differ from the reference program's by a relative error of at most 0.014.
Values may be sent and summed in bfloat16 or wider, within the bound.
A program may use at most 64 MiB of HBM per device.

```python
import math
import jax
import jax.numpy as jnp
import numpy as np
from jax import lax

D = 2048
CH = 512
FF = 2048
FS = 512
TOPK = 2
TOK_SP = 384
TOKENS = 3072
EXPERTS = 16
CAP = 96
N_SP = 8


def draw_residual(key, part):
    column = jnp.arange(D, dtype=jnp.float32) / (D - 1)
    column_scale = 0.5 * jnp.exp(column * math.log(6.0))
    values = jnp.clip(jax.random.normal(key, (TOKENS, D), jnp.float32), -6.0, 6.0)
    return (values * column_scale[None, :]).astype(jnp.bfloat16)


def shard_levels(own_key, extent, pieces, least, largest):
    def one(dim, shards_of):
        steps = jax.random.uniform(jax.random.fold_in(jax.random.fold_in(own_key, 6), dim), (shards_of,), jnp.float32, least / len(pieces), largest / len(pieces))
        return jnp.repeat(jnp.exp(steps), extent[dim] // shards_of).reshape((-1,) + (1,) * (len(extent) - dim - 1))

    gain = one(*pieces[0])
    for cut in pieces[1:]:
        gain = gain * one(*cut)
    return gain


def routed_block(rng, own, number, rows, amount, top, limit, slope):
    ranking = jax.random.permutation(rng, amount)
    packed, usual = portions_of(amount, rows * top, limit, slope, True), portions_of(amount, rows * top, limit, slope, False)
    places = jnp.arange(amount)

    def named(tallies, offset_by):
        used = int((tallies > 0).sum())
        fixed = max(1, used // 4)
        passed = fixed + (places - fixed + offset_by * (used - fixed)) % max(1, amount - fixed)
        return jnp.zeros((amount,), jnp.int32).at[ranking[jnp.where(places < fixed, places, passed)]].set(jnp.asarray(tallies, jnp.int32))

    tallies = jnp.where(number % 4 == 0, named(packed, number // 4), named(usual, number - number // 4 - 1))
    mixed = jax.random.permutation(jax.random.fold_in(own, 3), amount)
    donor, receiver = mixed[0:amount // 2 * 2:2], mixed[1:amount // 2 * 2:2]
    slack = jnp.minimum(tallies[donor] - 1, limit - tallies[receiver]) // 2
    slack = jnp.where((donor == ranking[0]) | (receiver == ranking[0]) | (tallies[receiver] == 0), 0, jnp.maximum(slack, 0))
    passed = jax.random.randint(jax.random.fold_in(own, 4), (amount // 2,), 0, 1 << 20) % (slack + 1)
    tallies = tallies.at[donor].add(-passed).at[receiver].add(passed)
    members = jnp.searchsorted(jnp.cumsum(tallies), jnp.arange(rows * top), side="right").astype(jnp.int32)
    listing = members.reshape(top, rows).T
    listing = listing[jax.random.permutation(jax.random.fold_in(own, 1), rows)]
    offset_by = jax.random.randint(jax.random.fold_in(own, 2), (rows, 1), 0, top)
    return jnp.take_along_axis(listing, (jnp.arange(top)[None, :] + offset_by) % top, axis=1)


def portions_of(amount, total, limit, slope, full):
    weights = [(1 << 20) // math.isqrt(standing ** slope) + 1 for standing in range(1, amount + 1)]
    largest = limit if full else min(limit, max(-(-total // amount), total * weights[0] // sum(weights)))
    least = 1 if total - largest >= amount - 1 else 0
    given, spare = [largest] + [least] * (amount - 1), total - largest - least * (amount - 1)
    while spare > 0:
        candidates = [i for i in range(1, amount) if given[i] < largest] or [i for i in range(1, amount) if given[i] < limit]
        whole, remaining = sum([weights[i] for i in candidates]), spare
        for i in candidates:
            extra = min(limit - given[i], max(1, remaining * weights[i] // whole), spare)
            given[i] = given[i] + extra
            spare = spare - extra
    return np.array(given)


def bell_draw(rng, extent, deviation, most, shards=(), kind=jnp.bfloat16):
    array = jax.random.normal(rng, extent, jnp.float32) * deviation
    if len(shards) > 0:
        array = shard_levels(rng, extent, shards, -0.22, 0.18) * array
    return jnp.clip(array, min=-most, max=most).astype(kind)


def setup_inputs(seed: int = 0) -> dict:
    seeds = jax.random.split(jax.random.key(seed), 16)
    outer_gate = bell_draw(seeds[0], (CH, TOKENS), 1.0, 6.0, ((0, 4), (1, 8)))
    inner_gate = bell_draw(seeds[1], (CH, TOKENS), 1.0, 6.0, ((0, 4), (1, 8)))
    conv_input = bell_draw(seeds[2], (CH, TOKENS), 1.0, 6.0, ((0, 4), (1, 8)))
    conv_taps = bell_draw(seeds[3], (3, CH), 3 ** -0.5, 3.5, ((1, 4),))
    mix_weight = bell_draw(seeds[4], (CH, D), CH ** -0.5, 0.25, ((1, 4),))
    residual = draw_residual(jax.random.fold_in(seeds[15], 71), 0)
    norm_gain = jnp.clip(1.0 + 0.18 * jax.random.normal(seeds[6], (D,), jnp.float32), 0.099609375, 1.8984375).astype(jnp.bfloat16)
    routes_keys = jax.random.split(jax.random.fold_in(seeds[7], 1), TOKENS // TOK_SP)
    routes_turns = jax.random.permutation(jax.random.fold_in(seeds[7], 3), TOKENS // TOK_SP)
    routes = jax.vmap(lambda own, number: routed_block(jax.random.fold_in(seeds[7], 2), own, number, TOK_SP, EXPERTS, TOPK, CAP, 2))(routes_keys, routes_turns).reshape((TOKENS, TOPK))
    route_scores = jnp.clip(0.05 + 0.95 * jax.random.uniform(seeds[8], (TOKENS, TOPK), jnp.float32) ** shard_levels(seeds[8], (TOKENS, TOPK), ((0, 8),), -0.2, 0.2), 0.05, 1.0)
    expert_gate = bell_draw(seeds[9], (EXPERTS, D, FF), D ** -0.5, 0.125, ((0, 8), (2, 4)))
    expert_up = bell_draw(seeds[10], (EXPERTS, D, FF), D ** -0.5, 0.125, ((0, 8), (2, 4)))
    expert_down = bell_draw(seeds[11], (EXPERTS, FF, D), FF ** -0.5, 0.125, ((0, 8), (2, 4)))
    shared_gate = bell_draw(seeds[12], (D, FS), D ** -0.5, 0.125, ((1, 4),))
    shared_up = bell_draw(seeds[13], (D, FS), D ** -0.5, 0.125, ((1, 4),))
    shared_down = bell_draw(seeds[14], (FS, D), FS ** -0.5, 0.25, ((1, 4),))
    return {"outer_gate": outer_gate, "inner_gate": inner_gate, "conv_input": conv_input, "conv_taps": conv_taps, "mix_weight": mix_weight, "residual": residual, "norm_gain": norm_gain, "routes": routes, "route_scores": route_scores, "expert_gate": expert_gate, "expert_up": expert_up, "expert_down": expert_down, "shared_gate": shared_gate, "shared_up": shared_up, "shared_down": shared_down}


epsilon = 1e-06
routed_scale = 2.5

def slot_tables(routes_block, expert_count, capacity):
    count_rows, top_count = routes_block.shape
    flat_route = routes_block.reshape(-1)
    onehot = (flat_route[:, None] == jnp.arange(expert_count, dtype=jnp.int32)[None, :]).astype(jnp.int32)
    before = jnp.cumsum(onehot, axis=0) - onehot
    position = lax.optimization_barrier(jnp.sum(before * onehot, axis=1)).astype(jnp.int32)
    slot_index = (flat_route * capacity + position).astype(jnp.int32)
    token_ids = (jnp.arange(count_rows * top_count, dtype=jnp.int32) // top_count).astype(jnp.int32)
    owners = jnp.full((expert_count * capacity,), -1, jnp.int32).at[slot_index].set(token_ids)
    return (slot_index.reshape(count_rows, top_count), owners)

def reference(outer_gate, inner_gate, conv_input, conv_taps, mix_weight, residual, norm_gain, routes, route_scores, expert_gate, expert_up, expert_down, shared_gate, shared_up, shared_down):
    product = (inner_gate.astype(jnp.float32) * conv_input.astype(jnp.float32)).astype(jnp.bfloat16)
    padded = jnp.pad(product.astype(jnp.float32), ((0, 0), (1, 1)))
    kernel = conv_taps.astype(jnp.float32)
    filtered = kernel[0][:, None] * padded[:, :-2] + kernel[1][:, None] * padded[:, 1:-1] + kernel[2][:, None] * padded[:, 2:]
    mixed = (outer_gate.astype(jnp.float32) * filtered).astype(jnp.bfloat16)
    projected = lax.dot_general(mixed, mix_weight, (((0,), (0,)), ((), ())), preferred_element_type=jnp.float32)
    stream = (residual.astype(jnp.float32) + projected).astype(jnp.bfloat16)
    levels = stream.astype(jnp.float32)
    inverse_rms = lax.rsqrt(lax.optimization_barrier(jnp.mean(levels * levels, axis=1)) + epsilon)
    normed = (levels * inverse_rms[:, None] * norm_gain.astype(jnp.float32)).astype(jnp.bfloat16)
    shared_act = (jax.nn.silu(jnp.dot(normed, shared_gate, preferred_element_type=jnp.float32)) * jnp.dot(normed, shared_up, preferred_element_type=jnp.float32)).astype(jnp.bfloat16)
    shared_out = jnp.dot(shared_act, shared_down, preferred_element_type=jnp.float32)
    blocks = routes.reshape(N_SP, TOK_SP, TOPK)
    slot_index, owners = jax.vmap(lambda block: slot_tables(block, EXPERTS, CAP))(blocks)
    offsets = (jnp.arange(N_SP, dtype=jnp.int32) * TOK_SP)[:, None]
    global_rows = jnp.where(owners >= 0, owners + offsets, -1).astype(jnp.int32)
    per_expert = global_rows.reshape(N_SP, EXPERTS, CAP).transpose(1, 0, 2).reshape(EXPERTS, N_SP * CAP)

    def run_expert(inputs):
        row_ids, gate_w, up_w, down_w = inputs
        filled = row_ids >= 0
        rows = jnp.where(filled[:, None], normed[jnp.maximum(row_ids, 0)], jnp.zeros((), jnp.bfloat16))
        gate_act = jnp.dot(rows, gate_w, preferred_element_type=jnp.float32)
        up_act = jnp.dot(rows, up_w, preferred_element_type=jnp.float32)
        hidden = (jax.nn.silu(gate_act) * up_act).astype(jnp.bfloat16)
        return jnp.dot(hidden, down_w, preferred_element_type=jnp.float32).astype(jnp.bfloat16)
    results = lax.map(run_expert, (per_expert, expert_gate, expert_up, expert_down))
    flat_results = results.reshape(EXPERTS * N_SP * CAP, D)
    chosen = routes.reshape(N_SP, TOK_SP, TOPK)
    position = slot_index - chosen * CAP
    block_ids = jnp.arange(N_SP, dtype=jnp.int32)[:, None, None]
    lookup = ((chosen * N_SP + block_ids) * CAP + position).astype(jnp.int32).reshape(TOKENS, TOPK)
    picked = flat_results[lookup].astype(jnp.float32)
    weights = route_scores / lax.optimization_barrier(jnp.sum(route_scores, axis=1, keepdims=True)) * routed_scale
    routed = lax.optimization_barrier(jnp.sum(weights[:, :, None] * picked, axis=1))
    return (stream.astype(jnp.float32) + routed + shared_out).astype(jnp.bfloat16)
```

```python
import functools

import jax
import jax.numpy as jnp
from jax import lax
from jax.experimental import pallas as pl
from jax.experimental.pallas import tpu as pltpu
from jax.sharding import PartitionSpec as P

D = 2048


epsilon = 1e-06
routed_scale = 2.5


MESH = pl.DeviceIdType.MESH
VMEM_LIMIT = 58 * 2**20


def moe_kernel(
    n_sp,
    n_tp,
    outer,
    inner,
    conv,
    taps,
    mix,
    residual,
    gain,
    routes_rows,
    scores,
    gate_hbm,
    up_hbm,
    down_hbm,
    sgate,
    sup,
    sdown,
    out,
    ret,
    shared_out,
    outgoing,
    extra,
    normed,
    stream,
    product,
    before,
    after,
    mixed,
    sums,
    recv,
    hid,
    whole,
    sact,
    obuf,
    gate_w,
    up_w,
    down_w,
    load_sem,
    own_sem,
    h_send,
    h_recv,
    a_send,
    a_recv,
    b_send,
    b_recv,
    y_send,
    y_recv,
    d_send,
    d_recv,
    f_send,
    f_recv,
    r_send,
    r_recv,
):
    s = lax.axis_index("sp")
    t = lax.axis_index("tp")
    rows_y = n_tp // 2
    y, c = t // 2, lax.rem(t, 2)
    partner = y * 2 + (1 - c)
    experts, cap, width = outgoing.shape[1:]
    hidden_width = gate_w.shape[2]
    shared_width = sgate.shape[1]
    DISPATCH, HIDDEN = 0, n_sp
    WHOLE, SHARED, MIXED, SUMS = 2 * n_sp, 2 * n_sp + 1, 2 * n_sp + 2, 2 * n_sp + 3
    channels, tokens_here = outer.shape
    expert_count = n_sp * experts
    f32 = jnp.float32

    half = n_sp // 2
    near = half if rows_y == 2 else 1
    order = list(range(1, near)) + list(range(near, n_sp))
    if near > 1:
        order = [half, half + 1, 1, *range(half + 2, n_sp), *range(2, near)]

    def chunk(i):
        return sum(jnp.where(i == p + 1, k, 0) for p, k in enumerate(order))

    def mate(k):
        total, bit = 0, 1
        while bit < n_sp:
            total = total + lax.rem(s // bit + k // bit, 2) * bit
            bit *= 2
        return total

    def y_peer(j):
        return lax.rem(y + j, rows_y) * 2

    def y_source(j):
        return lax.rem(y - j + rows_y, rows_y) * 2

    barrier = pltpu.get_barrier_semaphore()
    for j in range(1, n_sp):
        pl.semaphore_signal(barrier, inc=1, device_id=(mate(j), t), device_id_type=MESH)
    for j in range(1, rows_y):
        pl.semaphore_signal(barrier, inc=1, device_id=(s, y_peer(j) + c), device_id_type=MESH)
    pl.semaphore_signal(barrier, inc=1, device_id=(s, partner), device_id_type=MESH)

    filtered_input = inner[...].astype(f32) * conv[...].astype(f32)
    product[...] = filtered_input.astype(jnp.bfloat16)
    loads = [
        pltpu.make_async_copy(source, target, load_sem.at[i])
        for i, (source, target) in enumerate(((gate_hbm, gate_w), (up_hbm, up_w), (down_hbm, down_w)))
    ]
    for load in loads:
        load.start()
    pl.semaphore_wait(barrier, n_sp - 1 + rows_y - 1 + 1)

    def rows_of(k):
        return pl.ds(pl.multiple_of(mate(k) * cap, cap), cap)

    def block(k, owner):
        return recv.at[:, rows_of(k), pl.ds(pl.multiple_of(owner * width, width), width)]

    def hidden_block(k, owner):
        return hid.at[:, rows_of(k), pl.ds(pl.multiple_of(owner * hidden_width, hidden_width), hidden_width)]

    def whole_block(k, owner):
        return whole.at[:, pl.ds(pl.multiple_of(owner * width, width), width)]

    def shared_block(k, owner):
        return sact.at[owner]

    def remote(source, target, send, receive, device):
        return pltpu.make_async_remote_copy(
            src_ref=source,
            dst_ref=target,
            send_sem=send,
            recv_sem=receive,
            device_id=device,
            device_id_type=MESH,
        )

    def y_copy(view, k, slot, j):
        return remote(view(k, t), view(k, t), y_send.at[slot], y_recv.at[slot], (s, y_peer(j) + c))

    def d_copy(view, k, slot):
        return remote(view(k, t), view(k, t), d_send.at[slot], d_recv.at[slot], (s, partner))

    def f_copy(view, k, slot, j):
        ref = view(k, y_source(j) + c)
        return remote(ref, ref, f_send.at[slot], f_recv.at[slot], (s, partner))

    def spread(view, k, slot):
        for j in range(1, rows_y):
            y_copy(view, k, slot, j).start()
        d_copy(view, k, slot).start()

    def forward(view, k, slot):
        for j in range(1, rows_y):
            y_copy(view, k, slot, j).wait_recv()
        for j in range(1, rows_y):
            f_copy(view, k, slot, j).start()

    def collect(view, k, slot):
        d_copy(view, k, slot).wait_recv()
        for j in range(1, rows_y):
            f_copy(view, k, slot, j).wait_recv()

    def finish_sends(view, k, slot):
        for j in range(1, rows_y):
            y_copy(view, k, slot, j).wait_send()
            f_copy(view, k, slot, j).wait_send()
        d_copy(view, k, slot).wait_send()

    def a_copy(k):
        rows = pl.ds(pl.multiple_of(s * cap, cap), cap)
        columns = pl.ds(pl.multiple_of(t * width, width), width)
        return remote(
            outgoing.at[k], recv.at[:, rows, columns], a_send.at[k], a_recv.at[k], (mate(k), t)
        )

    def b_copy(k, j):
        rows = pl.ds(pl.multiple_of(s * cap, cap), cap)
        columns = pl.ds(pl.multiple_of((y_source(j) + c) * width, width), width)
        return remote(
            extra.at[k, j - 1], recv.at[:, rows, columns], b_send.at[k, j], b_recv.at[k, j], (mate(k), t)
        )

    def r_copy(k):
        return remote(obuf.at[k], ret.at[s], r_send.at[k], r_recv.at[k], (mate(k), t))

    def column_of(row):
        return jnp.broadcast_to(row, (128, row.shape[1])).T[:, 0:1]

    def mixed_block(k, owner):
        return mixed.at[pl.ds(pl.multiple_of(owner * channels, channels), channels), :]

    def sums_block(k, owner):
        return sums.at[owner]

    edge = before.shape[1]
    up_copy = remote(
        product.at[:, pl.ds(tokens_here - edge, edge)], before, h_send.at[0], h_recv.at[0],
        (lax.rem(s + 1, n_sp), t),
    )
    down_copy = remote(
        product.at[:, pl.ds(0, edge)], after, h_send.at[1], h_recv.at[1],
        (lax.rem(s + n_sp - 1, n_sp), t),
    )
    up_copy.start()
    down_copy.start()

    token_i = lax.broadcasted_iota(jnp.int32, (tokens_here, tokens_here), 0)
    token_j = lax.broadcasted_iota(jnp.int32, (tokens_here, tokens_here), 1)
    choices = routes_rows.shape[0]
    one_row = [
        (routes_rows[k : k + 1, :] == lax.broadcasted_iota(jnp.int32, (expert_count, tokens_here), 0)).astype(f32)
        for k in range(choices)
    ]
    earlier_row = jnp.dot(
        sum(one_row).astype(jnp.bfloat16), (token_i < token_j).astype(f32).astype(jnp.bfloat16),
        preferred_element_type=f32,
    )
    slot_row = [
        routes_rows[k : k + 1, :] * cap + jnp.sum(earlier_row * one_row[k], axis=0, keepdims=True).astype(jnp.int32)
        for k in range(choices)
    ]
    slot_column = [column_of(slot_row[k].astype(f32)).astype(jnp.int32) for k in range(choices)]

    up_copy.wait_recv()
    down_copy.wait_recv()
    values = product[...].astype(f32)
    place = lax.broadcasted_iota(jnp.int32, (channels, tokens_here), 1)
    first = jnp.where(s == 0, 0.0, before[...].astype(f32)[:, edge - 1 : edge])
    last = jnp.where(s == n_sp - 1, 0.0, after[...].astype(f32)[:, 0:1])
    previous = jnp.where(place == 0, first, pltpu.roll(values, 1, 1))
    following = jnp.where(place == tokens_here - 1, last, pltpu.roll(values, tokens_here - 1, 1))
    tap = taps[...].astype(f32)
    filtered = (
        column_of(tap[0:1]) * previous + column_of(tap[1:2]) * values + column_of(tap[2:3]) * following
    )
    mixed[pl.ds(pl.multiple_of(t * channels, channels), channels), :] = (
        outer[...].astype(f32) * filtered
    ).astype(jnp.bfloat16)
    spread(mixed_block, 0, MIXED)
    forward(mixed_block, 0, MIXED)
    collect(mixed_block, 0, MIXED)
    projected = lax.dot_general(
        mixed[...], mix[...], (((0,), (0,)), ((), ())), preferred_element_type=f32
    )
    stream[...] = (residual[...].astype(f32) + projected).astype(jnp.bfloat16)
    levels = stream[...].astype(f32)
    own = jnp.broadcast_to(jnp.sum(levels * levels, axis=1, keepdims=True), (tokens_here, 128))
    sums[t] = own.T[:8]
    spread(sums_block, 0, SUMS)
    forward(sums_block, 0, SUMS)
    collect(sums_block, 0, SUMS)
    squares = sums[0]
    for j in range(1, n_tp):
        squares = squares + sums[j]
    squares = jnp.broadcast_to(squares[0:1], (128, tokens_here)).T[:, 0:1]
    inverse_rms = lax.rsqrt(squares / D + epsilon)
    normed[...] = (levels * inverse_rms * gain[...].astype(f32)).astype(jnp.bfloat16)

    def picked(peer):
        spot = lax.broadcasted_iota(jnp.int32, (experts * cap, tokens_here), 0) + peer * (experts * cap)
        return sum((spot == slot_row[k]).astype(f32) for k in range(choices)).astype(jnp.bfloat16)

    def gathered(chosen, columns):
        return jnp.dot(chosen, columns, preferred_element_type=f32).astype(jnp.bfloat16)

    own_whole = pltpu.make_async_copy(normed, whole_block(0, t), own_sem)
    own_whole.start()
    own_whole.wait()
    spread(whole_block, 0, WHOLE)

    @pl.loop(1, n_sp)
    def _(q):
        k = 1 + lax.rem(q - 2 + half, n_sp - 1)
        packed = gathered(picked(mate(k)), normed[...])
        for e in range(experts):
            outgoing[k, e] = packed[e * cap : (e + 1) * cap]
        a_copy(k).start()

    forward(whole_block, 0, WHOLE)
    collect(whole_block, 0, WHOLE)

    def arrive(i):
        k = chunk(i)
        a_copy(k).wait_recv()

        @pl.when(k >= near)
        def _():
            spread(block, k, DISPATCH + k)

        @pl.when(k < near)
        def _():
            for j in range(1, rows_y):
                b_copy(k, j).wait_recv()
            d_copy(block, k, DISPATCH + k).start()
            for j in range(1, rows_y):
                f_copy(block, k, DISPATCH + k, j).start()

    def pass_on(i):
        k = chunk(i)

        @pl.when(k >= near)
        def _():
            forward(block, k, DISPATCH + k)

    def expert_in(k):
        rows = rows_of(k)
        columns = pl.ds(pl.multiple_of(t * hidden_width, hidden_width), hidden_width)
        for e in range(experts):
            x = recv[e, rows, :]
            gate = jnp.dot(x, gate_w[e], preferred_element_type=jnp.float32)
            up = jnp.dot(x, up_w[e], preferred_element_type=jnp.float32)
            hid[e, rows, columns] = (jax.nn.silu(gate) * up).astype(jnp.bfloat16)
        spread(hidden_block, k, HIDDEN + k)

    arrive(1)

    @pl.loop(1, near)
    def _(k):
        chosen = picked(mate(k))
        for j in range(1, rows_y):
            columns = pl.ds(pl.multiple_of((y_source(j) + c) * width, width), width)
            packed = gathered(chosen, whole[:, columns])
            for e in range(experts):
                extra[k, j - 1, e] = packed[e * cap : (e + 1) * cap]
            b_copy(k, j).start()

    own_rows = gathered(picked(s), whole[...])
    for e in range(experts):
        recv[e, rows_of(0), :] = own_rows[e * cap : (e + 1) * cap]
    for load in loads:
        load.wait()
    expert_in(0)
    tokens = whole[...]
    shared_hidden = jax.nn.silu(jnp.dot(tokens, sgate[...], preferred_element_type=jnp.float32)) * jnp.dot(
        tokens, sup[...], preferred_element_type=jnp.float32
    )
    sact[t] = shared_hidden.astype(jnp.bfloat16)
    spread(shared_block, 0, SHARED)

    weight_rows = scores[...] / jnp.sum(scores[...], axis=0, keepdims=True) * routed_scale
    weights = [column_of(weight_rows[k : k + 1]) for k in range(choices)]

    @pl.loop(2, n_sp + 6)
    def _(i):
        @pl.when((i >= 3) & (i < n_sp + 2))
        def _():
            k = chunk(i - 2)
            collect(block, k, DISPATCH + k)
            expert_in(k)

        @pl.when(i < n_sp)
        def _():
            arrive(i)

        @pl.when(i < n_sp + 1)
        def _():
            pass_on(i - 1)

        @pl.when((i >= 3) & (i < n_sp + 3))
        def _():
            k = chunk(i - 3)
            forward(hidden_block, k, HIDDEN + k)

        @pl.when((i >= 4) & (i < n_sp + 4))
        def _():
            k = chunk(i - 4)
            collect(hidden_block, k, HIDDEN + k)
            rows = rows_of(k)
            for e in range(experts):
                obuf[k, e] = jnp.dot(
                    hid[e, rows, :], down_w[e], preferred_element_type=jnp.float32
                ).astype(jnp.bfloat16)

            @pl.when(k > 0)
            def _():
                r_copy(k).start()

            @pl.when(k == 0)
            def _():
                ret[s] = obuf[0]

        @pl.when(i == 3)
        def _():
            forward(shared_block, 0, SHARED)

        @pl.when(i == 4)
        def _():
            collect(shared_block, 0, SHARED)
            total = jnp.zeros(shared_out.shape, jnp.float32)
            for j in range(n_tp):
                rows = sdown[pl.ds(j * shared_width, shared_width), :]
                total = total + jnp.dot(sact[j], rows, preferred_element_type=jnp.float32)
            shared_out[...] = total

        @pl.when(i >= 6)
        def _():
            k = chunk(i - 6)

            @pl.when(k > 0)
            def _():
                r_copy(k).wait_recv()

            group = mate(k)
            spot = lax.broadcasted_iota(jnp.int32, (tokens_here, experts * cap), 1) + group * (experts * cap)
            rows = ret[group].reshape(experts * cap, width)
            total = shared_out[...]
            for j in range(choices):
                chosen = (spot == slot_column[j]).astype(f32).astype(jnp.bfloat16)
                total = total + weights[j] * jnp.dot(chosen, rows, preferred_element_type=f32)
            shared_out[...] = total

    out[...] = (stream[...].astype(f32) + shared_out[...]).astype(jnp.bfloat16)

    up_copy.wait_send()
    down_copy.wait_send()
    finish_sends(mixed_block, 0, MIXED)
    finish_sends(sums_block, 0, SUMS)
    finish_sends(whole_block, 0, WHOLE)
    finish_sends(shared_block, 0, SHARED)

    finish_sends(hidden_block, 0, HIDDEN)

    @pl.loop(1, n_sp)
    def _(k):
        finish_sends(hidden_block, k, HIDDEN + k)
        a_copy(k).wait_send()
        r_copy(k).wait_send()

        @pl.when(k >= near)
        def _():
            finish_sends(block, k, DISPATCH + k)

        @pl.when(k < near)
        def _():
            d_copy(block, k, DISPATCH + k).wait_send()
            for j in range(1, rows_y):
                f_copy(block, k, DISPATCH + k, j).wait_send()
                b_copy(k, j).wait_send()


def local(
    outer_gate,
    inner_gate,
    conv_input,
    conv_taps,
    mix_weight,
    residual,
    norm_gain,
    routes,
    route_scores,
    expert_gate,
    expert_up,
    expert_down,
    shared_gate,
    shared_up,
    shared_down,
):
    n_sp, n_tp = lax.axis_size("sp"), lax.axis_size("tp")
    experts, depth, hidden_width = expert_gate.shape
    channels, token_count = outer_gate.shape
    width = residual.shape[1]
    cap = 2 * token_count * routes.shape[1] // (experts * n_sp)
    cap = (cap + 15) // 16 * 16
    slots = 2 * n_sp + 4
    edge = min(128, token_count)
    vmem = pl.BlockSpec(memory_space=pltpu.VMEM)
    hbm = pl.BlockSpec(memory_space=pl.ANY)
    bf16 = jnp.bfloat16
    dma = pltpu.SemaphoreType.DMA
    return pl.pallas_call(
        functools.partial(moe_kernel, n_sp, n_tp),
        name="moe",
        out_shape=jax.ShapeDtypeStruct((token_count, width), bf16),
        in_specs=[vmem] * 9 + [hbm] * 3 + [vmem] * 3,
        out_specs=vmem,
        scratch_shapes=[
            pltpu.VMEM((n_sp, experts, cap, width), bf16),
            pltpu.VMEM((token_count, width), jnp.float32),
            pltpu.VMEM((n_sp, experts, cap, width), bf16),
            pltpu.VMEM((n_sp // 2, n_tp // 2 - 1, experts, cap, width), bf16),
            pltpu.VMEM((token_count, width), bf16),
            pltpu.VMEM((token_count, width), bf16),
            pltpu.VMEM((channels, token_count), bf16),
            pltpu.VMEM((channels, edge), bf16),
            pltpu.VMEM((channels, edge), bf16),
            pltpu.VMEM((channels * n_tp, token_count), bf16),
            pltpu.VMEM((n_tp, 8, token_count), jnp.float32),
            pltpu.VMEM((experts, n_sp * cap, width * n_tp), bf16),
            pltpu.VMEM((experts, n_sp * cap, hidden_width * n_tp), bf16),
            pltpu.VMEM((token_count, width * n_tp), bf16),
            pltpu.VMEM((n_tp, token_count, shared_gate.shape[1]), bf16),
            pltpu.VMEM((n_sp, experts, cap, width), bf16),
            pltpu.VMEM(expert_gate.shape, bf16),
            pltpu.VMEM(expert_up.shape, bf16),
            pltpu.VMEM(expert_down.shape, bf16),
            dma((3,)),
            dma,
            dma((2,)),
            dma((2,)),
            dma((n_sp,)),
            dma((n_sp,)),
            dma((n_sp // 2, n_tp // 2)),
            dma((n_sp // 2, n_tp // 2)),
            dma((slots,)),
            dma((slots,)),
            dma((slots,)),
            dma((slots,)),
            dma((slots,)),
            dma((slots,)),
            dma((n_sp,)),
            dma((n_sp,)),
        ],
        compiler_params=pltpu.CompilerParams(
            collective_id=0, has_side_effects=True, vmem_limit_bytes=VMEM_LIMIT
        ),
    )(
        outer_gate,
        inner_gate,
        conv_input,
        conv_taps,
        mix_weight,
        residual,
        norm_gain.reshape(1, width),
        routes.T,
        route_scores.T,
        expert_gate,
        expert_up,
        expert_down,
        shared_gate,
        shared_up,
        shared_down,
    )


def solution(mesh):
    in_specs = (
        P("tp", "sp"),
        P("tp", "sp"),
        P("tp", "sp"),
        P(None, "tp"),
        P(None, "tp"),
        P("sp", "tp"),
        P("tp"),
        P("sp", None),
        P("sp", None),
        P("sp", None, "tp"),
        P("sp", None, "tp"),
        P("sp", None, "tp"),
        P(None, "tp"),
        P(None, "tp"),
        P(None, "tp"),
    )
    out_specs = P("sp", "tp")
    return jax.shard_map(local, mesh=mesh, in_specs=in_specs, out_specs=out_specs, check_vma=False)
```

```python
import functools

import jax
import jax.numpy as jnp
from jax import lax
from jax.experimental import pallas as pl
from jax.experimental.pallas import tpu as pltpu
from jax.sharding import PartitionSpec as P

D = 2048


epsilon = 1e-06
routed_scale = 2.5


MESH = pl.DeviceIdType.MESH
VMEM_LIMIT = 58 * 2**20


def moe_kernel(
    n_sp,
    n_tp,
    outer_hbm,
    inner_hbm,
    conv_hbm,
    taps_hbm,
    gain_hbm,
    routes_hbm,
    scores_hbm,
    mix_hbm,
    residual_hbm,
    gate_hbm,
    up_hbm,
    down_hbm,
    sgate_hbm,
    sup_hbm,
    sdown_hbm,
    out,
    ret,
    shared_out,
    outgoing,
    extra,
    normed,
    stream,
    product,
    before,
    after,
    mixed,
    sums,
    gains,
    gain_row,
    inverse_out,
    inverse_in,
    own_inverse,
    far_inverse,
    far_routes,
    far_stream,
    recv,
    hid,
    whole,
    sact,
    obuf,
    outer,
    inner,
    conv,
    taps,
    gain,
    routes_rows,
    scores,
    mix,
    residual,
    gate_w,
    up_w,
    down_w,
    sgate,
    sup,
    sdown,
    load_sem,
    own_sem,
    h_send,
    h_recv,
    a_send,
    a_recv,
    b_send,
    b_recv,
    i_send,
    i_recv,
    p_send,
    p_recv,
    y_send,
    y_recv,
    d_send,
    d_recv,
    f_send,
    f_recv,
    r_send,
    r_recv,
):
    s = lax.axis_index("sp")
    t = lax.axis_index("tp")
    rows_y = n_tp // 2
    y, c = t // 2, lax.rem(t, 2)
    partner = y * 2 + (1 - c)
    experts, cap, width = outgoing.shape[1:]
    hidden_width = gate_w.shape[2]
    shared_width = sgate.shape[1]
    DISPATCH, HIDDEN = 0, n_sp
    WHOLE, SHARED, MIXED, SUMS, GAINS = (2 * n_sp + j for j in range(5))
    channels, tokens_here = outer.shape
    expert_count = n_sp * experts
    f32 = jnp.float32

    half = n_sp // 2
    near = half if rows_y == 2 else 2
    quarter = half // 2
    central = lax.rem((s // quarter + 1) // 2, 2)
    order = [1, half, *range(2, half), *range(half + 1, n_sp)]
    outer_order = order
    combine = [0, *order]
    if near > 2:
        late = list(range(half + 2, n_sp))
        order = [1, half, half + 1, *late, *range(2, near)]
        outer_order = [1, half, *late, half + 1, *range(2, near)]
        combine = [0, 1, half, late[0], half + 1, *late[1:], *range(2, near)]

    def whole_rows(k):
        return (k > 1) & (k < near)

    def entry(table, i):
        return sum(jnp.where(i == p, k, 0) for p, k in enumerate(table))

    def chunk(i):
        return central * entry([0, *order], i) + (1 - central) * entry([0, *outer_order], i)

    def mate(k):
        total, bit = 0, 1
        while bit < n_sp:
            total = total + lax.rem(s // bit + k // bit, 2) * bit
            bit *= 2
        return total

    def y_peer(j):
        return lax.rem(y + j, rows_y) * 2

    def y_source(j):
        return lax.rem(y - j + rows_y, rows_y) * 2

    barrier = pltpu.get_barrier_semaphore()
    for j in range(1, n_sp):
        pl.semaphore_signal(barrier, inc=1, device_id=(mate(j), t), device_id_type=MESH)
    for j in range(1, rows_y):
        pl.semaphore_signal(barrier, inc=1, device_id=(s, y_peer(j) + c), device_id_type=MESH)
    pl.semaphore_signal(barrier, inc=1, device_id=(s, partner), device_id_type=MESH)

    places = (
        (inner_hbm, inner),
        (conv_hbm, conv),
        (gain_hbm, gain),
        (routes_hbm, routes_rows),
        (outer_hbm, outer),
        (taps_hbm, taps),
        (scores_hbm, scores),
        (mix_hbm, mix),
        (residual_hbm, residual),
        (gate_hbm, gate_w),
        (up_hbm, up_w),
        (down_hbm, down_w),
        (sgate_hbm, sgate),
        (sup_hbm, sup),
        (sdown_hbm, sdown),
    )
    loads = [pltpu.make_async_copy(source, target, load_sem.at[i]) for i, (source, target) in enumerate(places)]
    for load in loads:
        load.start()
    for load in loads[:4]:
        load.wait()
    filtered_input = inner[...].astype(f32) * conv[...].astype(f32)
    product[...] = filtered_input.astype(jnp.bfloat16)
    gains[t] = jnp.broadcast_to(gain[...].astype(f32).reshape(1, width), gains.shape[1:])
    pl.semaphore_wait(barrier, n_sp - 1 + rows_y - 1 + 1)

    def rows_of(k):
        return pl.ds(pl.multiple_of(mate(k) * cap, cap), cap)

    def block(k, owner):
        return recv.at[:, rows_of(k), pl.ds(pl.multiple_of(owner * width, width), width)]

    def hidden_block(k, owner):
        return hid.at[:, rows_of(k), pl.ds(pl.multiple_of(owner * hidden_width, hidden_width), hidden_width)]

    def whole_block(k, owner):
        return whole.at[:, pl.ds(pl.multiple_of(owner * width, width), width)]

    def shared_block(k, owner):
        return sact.at[owner]

    def remote(source, target, send, receive, device):
        return pltpu.make_async_remote_copy(
            src_ref=source,
            dst_ref=target,
            send_sem=send,
            recv_sem=receive,
            device_id=device,
            device_id_type=MESH,
        )

    def y_copy(view, k, slot, j):
        return remote(view(k, t), view(k, t), y_send.at[slot], y_recv.at[slot], (s, y_peer(j) + c))

    def d_copy(view, k, slot):
        return remote(view(k, t), view(k, t), d_send.at[slot], d_recv.at[slot], (s, partner))

    def f_copy(view, k, slot, j):
        ref = view(k, y_source(j) + c)
        return remote(ref, ref, f_send.at[slot], f_recv.at[slot], (s, partner))

    def spread(view, k, slot):
        for j in range(1, rows_y):
            y_copy(view, k, slot, j).start()
        d_copy(view, k, slot).start()

    def forward(view, k, slot):
        for j in range(1, rows_y):
            y_copy(view, k, slot, j).wait_recv()
        for j in range(1, rows_y):
            f_copy(view, k, slot, j).start()

    def collect(view, k, slot):
        d_copy(view, k, slot).wait_recv()
        for j in range(1, rows_y):
            f_copy(view, k, slot, j).wait_recv()

    def finish_sends(view, k, slot):
        for j in range(1, rows_y):
            y_copy(view, k, slot, j).wait_send()
            f_copy(view, k, slot, j).wait_send()
        d_copy(view, k, slot).wait_send()

    def a_copy(k):
        columns = pl.ds(pl.multiple_of(t * width, width), width)
        relayed = k // half
        source = mate(relayed * half)
        rows = pl.ds(pl.multiple_of(source * cap, cap), cap)
        return remote(
            outgoing.at[k], recv.at[:, rows, columns], a_send.at[k], a_recv.at[k], (mate(k - relayed * half), t)
        )

    def b_copy(k, j):
        rows = pl.ds(pl.multiple_of(s * cap, cap), cap)
        columns = pl.ds(pl.multiple_of((y_source(j) + c) * width, width), width)
        return remote(
            extra.at[k, j - 1], recv.at[:, rows, columns], b_send.at[k, j], b_recv.at[k, j], (mate(k), t)
        )

    def i_copy(k):
        return remote(inverse_out.at[k], inverse_in.at[k], i_send.at[k], i_recv.at[k], (mate(k - k // half * half), t))

    def p_copy(i, source, target):
        return remote(source, target, p_send.at[i], p_recv.at[i], (mate(half), t))

    routes_copy = p_copy(0, routes_rows, far_routes)
    stream_copy = p_copy(1, stream, far_stream)
    inverse_copy = p_copy(2, own_inverse, far_inverse)

    def r_copy(k):
        return remote(obuf.at[k], ret.at[s], r_send.at[k], r_recv.at[k], (mate(k), t))

    def column_of(row):
        return jnp.broadcast_to(row, (128, row.shape[1])).T[:, 0:1]

    def mixed_block(k, owner):
        return mixed.at[pl.ds(pl.multiple_of(owner * channels, channels), channels), :]

    def sums_block(k, owner):
        return sums.at[owner]

    def gains_block(k, owner):
        return gains.at[owner]

    edge = before.shape[1]
    up_copy = remote(
        product.at[:, pl.ds(tokens_here - edge, edge)], before, h_send.at[0], h_recv.at[0],
        (lax.rem(s + 1, n_sp), t),
    )
    down_copy = remote(
        product.at[:, pl.ds(0, edge)], after, h_send.at[1], h_recv.at[1],
        (lax.rem(s + n_sp - 1, n_sp), t),
    )
    up_copy.start()
    down_copy.start()
    spread(gains_block, 0, GAINS)
    routes_copy.start()

    token_i = lax.broadcasted_iota(jnp.int32, (tokens_here, tokens_here), 0)
    token_j = lax.broadcasted_iota(jnp.int32, (tokens_here, tokens_here), 1)
    choices = routes_rows.shape[0]

    def slots_of(routes):
        one_row = [
            (routes[k : k + 1, :] == lax.broadcasted_iota(jnp.int32, (expert_count, tokens_here), 0)).astype(f32)
            for k in range(choices)
        ]
        earlier_row = jnp.dot(
            sum(one_row).astype(jnp.bfloat16), (token_i < token_j).astype(f32).astype(jnp.bfloat16),
            preferred_element_type=f32,
        )
        rows = [
            routes[k : k + 1, :] * cap + jnp.sum(earlier_row * one_row[k], axis=0, keepdims=True).astype(jnp.int32)
            for k in range(choices)
        ]
        return rows, [column_of(row.astype(f32)).astype(jnp.int32) for row in rows]

    slot_row, slot_column = slots_of(routes_rows[...])

    for load in loads[4:7]:
        load.wait()
    up_copy.wait_recv()
    down_copy.wait_recv()
    values = product[...].astype(f32)
    place = lax.broadcasted_iota(jnp.int32, (channels, tokens_here), 1)
    first = jnp.where(s == 0, 0.0, before[...].astype(f32)[:, edge - 1 : edge])
    last = jnp.where(s == n_sp - 1, 0.0, after[...].astype(f32)[:, 0:1])
    previous = jnp.where(place == 0, first, pltpu.roll(values, 1, 1))
    following = jnp.where(place == tokens_here - 1, last, pltpu.roll(values, tokens_here - 1, 1))
    tap = taps[...].astype(f32)
    filtered = (
        column_of(tap[0:1]) * previous + column_of(tap[1:2]) * values + column_of(tap[2:3]) * following
    )
    mixed[pl.ds(pl.multiple_of(t * channels, channels), channels), :] = (
        outer[...].astype(f32) * filtered
    ).astype(jnp.bfloat16)
    spread(mixed_block, 0, MIXED)
    forward(mixed_block, 0, MIXED)
    collect(mixed_block, 0, MIXED)
    for load in loads[7:9]:
        load.wait()
    projected = lax.dot_general(
        mixed[...], mix[...], (((0,), (0,)), ((), ())), preferred_element_type=f32
    )
    stream[...] = (residual[...].astype(f32) + projected).astype(jnp.bfloat16)
    levels = stream[...].astype(f32)
    own = jnp.broadcast_to(jnp.sum(levels * levels, axis=1, keepdims=True), (tokens_here, 128))
    sums[t] = own.T[:8]
    spread(sums_block, 0, SUMS)
    def picked(peer, slots):
        spot = lax.broadcasted_iota(jnp.int32, (experts * cap, tokens_here), 0) + peer * (experts * cap)
        return sum((spot == slots[k]).astype(f32) for k in range(choices)).astype(jnp.bfloat16)

    def gathered(chosen, columns):
        return jnp.dot(chosen, columns, preferred_element_type=f32).astype(jnp.bfloat16)

    def pack(k, peer, slots, values):
        packed = gathered(picked(peer, slots), values)
        for e in range(experts):
            outgoing[k, e] = packed[e * cap : (e + 1) * cap]
        a_copy(k).start()

    stream_copy.start()
    own_whole = pltpu.make_async_copy(stream, whole_block(0, t), own_sem)
    own_whole.start()
    own_whole.wait()
    spread(whole_block, 0, WHOLE)

    @pl.loop(1, half)
    def _(k):
        pack(k, mate(k), slot_row, stream[...])

    routes_copy.wait_recv()
    far_row, far_column = slots_of(far_routes[...])
    forward(gains_block, 0, GAINS)
    forward(sums_block, 0, SUMS)
    collect(gains_block, 0, GAINS)
    for j in range(n_tp):
        gain_row[:, j * width : (j + 1) * width] = gains[j]
    collect(sums_block, 0, SUMS)
    squares = sums[0]
    for j in range(1, n_tp):
        squares = squares + sums[j]
    inverse_row = lax.rsqrt(squares[0:1] / D + epsilon)
    own_inverse[...] = jnp.broadcast_to(inverse_row, own_inverse.shape)
    inverse_copy.start()
    inverse_rms = column_of(inverse_row)

    def inverses(peer, slots, values):
        spot = lax.broadcasted_iota(jnp.int32, (tokens_here, inverse_in.shape[2]), 1) + peer * (experts * cap)
        hits = sum(jnp.where(spot == slots[k], values, 0.0) for k in range(choices))
        return jnp.broadcast_to(jnp.sum(hits, axis=0, keepdims=True), inverse_in.shape[1:])

    inverse_in[0] = inverses(s, slot_column, inverse_rms)

    @pl.loop(1, half)
    def _(k):
        inverse_out[k] = inverses(mate(k), slot_column, inverse_rms)
        i_copy(k).start()

    def arrive(i):
        k = chunk(i)
        a_copy(k).wait_recv()

        @pl.when(jnp.logical_not(whole_rows(k)))
        def _():
            spread(block, k, DISPATCH + k)

        @pl.when(whole_rows(k))
        def _():
            for j in range(1, rows_y):
                b_copy(k, j).wait_recv()
            d_copy(block, k, DISPATCH + k).start()
            for j in range(1, rows_y):
                f_copy(block, k, DISPATCH + k, j).start()

    def pass_on(i):
        k = chunk(i)

        @pl.when(jnp.logical_not(whole_rows(k)))
        def _():
            forward(block, k, DISPATCH + k)

    arrive(1)
    forward(whole_block, 0, WHOLE)
    collect(whole_block, 0, WHOLE)

    def expert_in(k):
        rows = rows_of(k)
        columns = pl.ds(pl.multiple_of(t * hidden_width, hidden_width), hidden_width)
        inverse = column_of(inverse_in[k][0:1])
        for e in range(experts):
            x = recv[e, rows, :].astype(f32) * inverse[e * cap : (e + 1) * cap] * gain_row[0:1]
            x = x.astype(jnp.bfloat16)
            gate = jnp.dot(x, gate_w[e], preferred_element_type=jnp.float32)
            up = jnp.dot(x, up_w[e], preferred_element_type=jnp.float32)
            hid[e, rows, columns] = (jax.nn.silu(gate) * up).astype(jnp.bfloat16)
        spread(hidden_block, k, HIDDEN + k)

    own_rows = gathered(picked(s, slot_row), whole[...])
    for e in range(experts):
        recv[e, rows_of(0), :] = own_rows[e * cap : (e + 1) * cap]
    for load in loads[9:]:
        load.wait()
    expert_in(0)

    def pack_extra(k):
        chosen = picked(mate(k), slot_row)
        for j in range(1, rows_y):
            columns = pl.ds(pl.multiple_of((y_source(j) + c) * width, width), width)
            packed = gathered(chosen, whole[:, columns])
            for e in range(experts):
                extra[k, j - 1, e] = packed[e * cap : (e + 1) * cap]
            b_copy(k, j).start()

    def take(i):
        k = chunk(i)
        pass_on(i)

        @pl.when(k != half)
        def _():
            i_copy(k).wait_recv()

        collect(block, k, DISPATCH + k)
        expert_in(k)

    take(1)
    stream_copy.wait_recv()

    @pl.loop(half + 1, n_sp)
    def _(k):
        pack(k, mate(k - half), far_row, far_stream[...])

    far_rows = gathered(picked(s, far_row), far_stream[...])
    for e in range(experts):
        recv[e, rows_of(half), pl.ds(pl.multiple_of(t * width, width), width)] = far_rows[e * cap : (e + 1) * cap]
    spread(block, half, DISPATCH + half)
    @pl.loop(2, near)
    def _(k):
        pack_extra(k)

    normed[...] = (whole[...].astype(f32) * inverse_rms * gain_row[0:1]).astype(jnp.bfloat16)
    tokens = normed[...]
    shared_hidden = jax.nn.silu(jnp.dot(tokens, sgate[...], preferred_element_type=jnp.float32)) * jnp.dot(
        tokens, sup[...], preferred_element_type=jnp.float32
    )
    sact[t] = shared_hidden.astype(jnp.bfloat16)
    spread(shared_block, 0, SHARED)

    inverse_copy.wait_recv()
    far_rms = column_of(far_inverse[0:1])
    inverse_in[half] = inverses(s, far_column, far_rms)

    @pl.loop(half + 1, n_sp)
    def _(k):
        inverse_out[k] = inverses(mate(k - half), far_column, far_rms)
        i_copy(k).start()

    weight_rows = scores[...] / jnp.sum(scores[...], axis=0, keepdims=True) * routed_scale
    weights = [column_of(weight_rows[k : k + 1]) for k in range(choices)]

    @pl.loop(2, n_sp + 7)
    def _(i):
        @pl.when((i > 2) & (i < n_sp))
        def _():
            arrive(i)

        @pl.when((i > 2) & (i < n_sp + 1))
        def _():
            take(i - 1)

        @pl.when(i < n_sp + 2)
        def _():
            k = chunk(i - 2)
            forward(hidden_block, k, HIDDEN + k)
            collect(hidden_block, k, HIDDEN + k)
            rows = rows_of(k)
            for e in range(experts):
                obuf[k, e] = jnp.dot(
                    hid[e, rows, :], down_w[e], preferred_element_type=jnp.float32
                ).astype(jnp.bfloat16)

            @pl.when(k > 0)
            def _():
                r_copy(k).start()

            @pl.when(k == 0)
            def _():
                ret[s] = obuf[0]

        @pl.when(i == 3)
        def _():
            forward(shared_block, 0, SHARED)

        @pl.when(i == 4)
        def _():
            collect(shared_block, 0, SHARED)
            total = jnp.zeros(shared_out.shape, jnp.float32)
            for j in range(n_tp):
                rows = sdown[pl.ds(j * shared_width, shared_width), :]
                total = total + jnp.dot(sact[j], rows, preferred_element_type=jnp.float32)
            shared_out[...] = total

        @pl.when(i >= 7)
        def _():
            k = entry(combine, i - 7)

            @pl.when(k > 0)
            def _():
                r_copy(k).wait_recv()

            group = mate(k)
            spot = lax.broadcasted_iota(jnp.int32, (tokens_here, experts * cap), 1) + group * (experts * cap)
            rows = ret[group].reshape(experts * cap, width)
            total = shared_out[...]
            for j in range(choices):
                chosen = (spot == slot_column[j]).astype(f32).astype(jnp.bfloat16)
                total = total + weights[j] * jnp.dot(chosen, rows, preferred_element_type=f32)
            shared_out[...] = total

    out[...] = (stream[...].astype(f32) + shared_out[...]).astype(jnp.bfloat16)

    routes_copy.wait_send()
    stream_copy.wait_send()
    inverse_copy.wait_send()
    up_copy.wait_send()
    down_copy.wait_send()
    finish_sends(mixed_block, 0, MIXED)
    finish_sends(sums_block, 0, SUMS)
    finish_sends(gains_block, 0, GAINS)
    finish_sends(whole_block, 0, WHOLE)
    finish_sends(shared_block, 0, SHARED)

    finish_sends(hidden_block, 0, HIDDEN)

    @pl.loop(1, n_sp)
    def _(k):
        finish_sends(hidden_block, k, HIDDEN + k)
        r_copy(k).wait_send()

        @pl.when(k != half)
        def _():
            a_copy(k).wait_send()
            i_copy(k).wait_send()

        @pl.when(jnp.logical_not(whole_rows(k)))
        def _():
            finish_sends(block, k, DISPATCH + k)

        @pl.when(whole_rows(k))
        def _():
            d_copy(block, k, DISPATCH + k).wait_send()
            for j in range(1, rows_y):
                f_copy(block, k, DISPATCH + k, j).wait_send()
                b_copy(k, j).wait_send()


def local(
    outer_gate,
    inner_gate,
    conv_input,
    conv_taps,
    mix_weight,
    residual,
    norm_gain,
    routes,
    route_scores,
    expert_gate,
    expert_up,
    expert_down,
    shared_gate,
    shared_up,
    shared_down,
):
    n_sp, n_tp = lax.axis_size("sp"), lax.axis_size("tp")
    experts, depth, hidden_width = expert_gate.shape
    channels, token_count = outer_gate.shape
    width = residual.shape[1]
    cap = 2 * token_count * routes.shape[1] // (experts * n_sp)
    cap = (cap + 15) // 16 * 16
    slots = 2 * n_sp + 5
    edge = min(128, token_count)
    lanes = (experts * cap + 127) // 128 * 128
    vmem = pl.BlockSpec(memory_space=pltpu.VMEM)
    hbm = pl.BlockSpec(memory_space=pltpu.HBM)
    bf16 = jnp.bfloat16
    dma = pltpu.SemaphoreType.DMA
    return pl.pallas_call(
        functools.partial(moe_kernel, n_sp, n_tp),
        name="moe",
        out_shape=pltpu.VMEM((token_count, width), bf16),
        in_specs=[hbm] * 15,
        out_specs=vmem,
        scratch_shapes=[
            pltpu.VMEM((n_sp, experts, cap, width), bf16),
            pltpu.VMEM((token_count, width), jnp.float32),
            pltpu.VMEM((n_sp, experts, cap, width), bf16),
            pltpu.VMEM((n_sp // 2, n_tp // 2 - 1, experts, cap, width), bf16),
            pltpu.VMEM((token_count, width * n_tp), bf16),
            pltpu.VMEM((token_count, width), bf16),
            pltpu.VMEM((channels, token_count), bf16),
            pltpu.VMEM((channels, edge), bf16),
            pltpu.VMEM((channels, edge), bf16),
            pltpu.VMEM((channels * n_tp, token_count), bf16),
            pltpu.VMEM((n_tp, 8, token_count), jnp.float32),
            pltpu.VMEM((n_tp, 8, width), jnp.float32),
            pltpu.VMEM((8, width * n_tp), jnp.float32),
            pltpu.VMEM((n_sp, 8, lanes), jnp.float32),
            pltpu.VMEM((n_sp, 8, lanes), jnp.float32),
            pltpu.VMEM((8, token_count), jnp.float32),
            pltpu.VMEM((8, token_count), jnp.float32),
            pltpu.VMEM((routes.shape[1], token_count), jnp.int32),
            pltpu.VMEM((token_count, width), bf16),
            pltpu.VMEM((experts, n_sp * cap, width * n_tp), bf16),
            pltpu.VMEM((experts, n_sp * cap, hidden_width * n_tp), bf16),
            pltpu.VMEM((token_count, width * n_tp), bf16),
            pltpu.VMEM((n_tp, token_count, shared_gate.shape[1]), bf16),
            pltpu.VMEM((n_sp, experts, cap, width), bf16),
            pltpu.VMEM(outer_gate.shape, bf16),
            pltpu.VMEM(inner_gate.shape, bf16),
            pltpu.VMEM(conv_input.shape, bf16),
            pltpu.VMEM(conv_taps.shape, bf16),
            pltpu.VMEM(norm_gain.shape, bf16),
            pltpu.VMEM(routes.shape[::-1], jnp.int32),
            pltpu.VMEM(route_scores.shape[::-1], jnp.float32),
            pltpu.VMEM(mix_weight.shape, bf16),
            pltpu.VMEM(residual.shape, bf16),
            pltpu.VMEM(expert_gate.shape, bf16),
            pltpu.VMEM(expert_up.shape, bf16),
            pltpu.VMEM(expert_down.shape, bf16),
            pltpu.VMEM(shared_gate.shape, bf16),
            pltpu.VMEM(shared_up.shape, bf16),
            pltpu.VMEM(shared_down.shape, bf16),
            dma((15,)),
            dma,
            dma((2,)),
            dma((2,)),
            dma((n_sp,)),
            dma((n_sp,)),
            dma((n_sp // 2, n_tp // 2)),
            dma((n_sp // 2, n_tp // 2)),
            dma((n_sp,)),
            dma((n_sp,)),
            dma((3,)),
            dma((3,)),
            dma((slots,)),
            dma((slots,)),
            dma((slots,)),
            dma((slots,)),
            dma((slots,)),
            dma((slots,)),
            dma((n_sp,)),
            dma((n_sp,)),
        ],
        compiler_params=pltpu.CompilerParams(
            collective_id=0, has_side_effects=True, vmem_limit_bytes=VMEM_LIMIT
        ),
    )(
        outer_gate,
        inner_gate,
        conv_input,
        conv_taps,
        norm_gain,
        routes.T,
        route_scores.T,
        mix_weight,
        residual,
        expert_gate,
        expert_up,
        expert_down,
        shared_gate,
        shared_up,
        shared_down,
    )


def solution(mesh):
    in_specs = (
        P("tp", "sp"),
        P("tp", "sp"),
        P("tp", "sp"),
        P(None, "tp"),
        P(None, "tp"),
        P("sp", "tp"),
        P("tp"),
        P("sp", None),
        P("sp", None),
        P("sp", None, "tp"),
        P("sp", None, "tp"),
        P("sp", None, "tp"),
        P(None, "tp"),
        P(None, "tp"),
        P(None, "tp"),
    )
    out_specs = P("sp", "tp")
    return jax.shard_map(local, mesh=mesh, in_specs=in_specs, out_specs=out_specs, check_vma=False)
```

```python
import functools

import jax
import jax.numpy as jnp
from jax import lax
from jax.experimental import pallas as pl
from jax.experimental.pallas import tpu as pltpu
from jax.sharding import PartitionSpec as P

D = 2048


epsilon = 1e-06
routed_scale = 2.5


MESH = pl.DeviceIdType.MESH
VMEM_LIMIT = 58 * 2**20


def moe_kernel(
    n_sp,
    n_tp,
    outer_hbm,
    inner_hbm,
    conv_hbm,
    taps_hbm,
    gain_hbm,
    routes_hbm,
    scores_hbm,
    mix_hbm,
    residual_hbm,
    gate_hbm,
    up_hbm,
    down_hbm,
    sgate_hbm,
    sup_hbm,
    sdown_hbm,
    out,
    ret,
    shared_out,
    outgoing,
    extra,
    normed,
    stream,
    product,
    before,
    after,
    mixed,
    edges,
    patched,
    sums,
    gains,
    gain_row,
    inverse_out,
    inverse_in,
    own_inverse,
    far_inverse,
    far_routes,
    far_stream,
    recv,
    hid,
    whole,
    sact,
    obuf,
    outer,
    inner,
    conv,
    taps,
    gain,
    routes_rows,
    scores,
    mix,
    residual,
    gate_w,
    up_w,
    down_w,
    sgate,
    sup,
    sdown,
    load_sem,
    own_sem,
    h_send,
    h_recv,
    a_send,
    a_recv,
    b_send,
    b_recv,
    i_send,
    i_recv,
    p_send,
    p_recv,
    y_send,
    y_recv,
    d_send,
    d_recv,
    f_send,
    f_recv,
    r_send,
    r_recv,
):
    s = lax.axis_index("sp")
    t = lax.axis_index("tp")
    rows_y = n_tp // 2
    y, c = t // 2, lax.rem(t, 2)
    partner = y * 2 + (1 - c)
    experts, cap, width = outgoing.shape[1:]
    hidden_width = gate_w.shape[2]
    shared_width = sgate.shape[1]
    DISPATCH, HIDDEN = 0, n_sp
    WHOLE, SHARED, MIXED, SUMS, GAINS, EDGES = (n_sp * (1 + experts) + j for j in range(6))
    channels, tokens_here = outer.shape
    expert_count = n_sp * experts
    f32 = jnp.float32

    half = n_sp // 2
    near = half if rows_y == 2 else 2
    quarter = half // 2
    central = lax.rem((s // quarter + 1) // 2, 2)
    order = [1, half, *range(2, half), *range(half + 1, n_sp)]
    outer_order = order
    combine = [0, *order]
    if near > 2:
        late = list(range(half + 2, n_sp))
        nearest = list(range(2, near))
        order = [1, half, half + 1, *late, *nearest]
        outer_order = [1, half, *late, half + 1, *nearest]
        combine = [0, 1, half, late[0], half + 1, *late[1:], *nearest]

    def whole_rows(k):
        return (k > 1) & (k < near)

    def entry(table, i):
        return sum(jnp.where(i == p, k, 0) for p, k in enumerate(table))

    def chunk(i):
        return central * entry([0, *order], i) + (1 - central) * entry([0, *outer_order], i)

    def mate(k):
        total, bit = 0, 1
        while bit < n_sp:
            total = total + lax.rem(s // bit + k // bit, 2) * bit
            bit *= 2
        return total

    def y_peer(j):
        return lax.rem(y + j, rows_y) * 2

    def y_source(j):
        return lax.rem(y - j + rows_y, rows_y) * 2

    barrier = pltpu.get_barrier_semaphore()
    for j in range(1, n_sp):
        pl.semaphore_signal(barrier, inc=1, device_id=(mate(j), t), device_id_type=MESH)
    for j in range(1, rows_y):
        pl.semaphore_signal(barrier, inc=1, device_id=(s, y_peer(j) + c), device_id_type=MESH)
    pl.semaphore_signal(barrier, inc=1, device_id=(s, partner), device_id_type=MESH)

    places = (
        (inner_hbm, inner),
        (conv_hbm, conv),
        (gain_hbm, gain),
        (routes_hbm, routes_rows),
        (outer_hbm, outer),
        (taps_hbm, taps),
        (scores_hbm, scores),
        (mix_hbm, mix),
        (residual_hbm, residual),
        (gate_hbm, gate_w),
        (up_hbm, up_w),
        (down_hbm, down_w),
        (sgate_hbm, sgate),
        (sup_hbm, sup),
        (sdown_hbm, sdown),
    )
    loads = [pltpu.make_async_copy(source, target, load_sem.at[i]) for i, (source, target) in enumerate(places)]
    for load in loads:
        load.start()
    for load in loads[:4]:
        load.wait()
    filtered_input = inner[...].astype(f32) * conv[...].astype(f32)
    product[...] = filtered_input.astype(jnp.bfloat16)
    gains[t] = jnp.broadcast_to(gain[...].astype(f32).reshape(1, width), gains.shape[1:])
    pl.semaphore_wait(barrier, n_sp - 1 + rows_y - 1 + 1)

    def rows_of(k):
        return pl.ds(pl.multiple_of(mate(k) * cap, cap), cap)

    def block(k, owner):
        return recv.at[:, rows_of(k), pl.ds(pl.multiple_of(owner * width, width), width)]

    def hidden_block(e):
        def view(k, owner):
            columns = pl.ds(pl.multiple_of(owner * hidden_width, hidden_width), hidden_width)
            return hid.at[e, rows_of(k), columns]

        return view

    def whole_block(k, owner):
        return whole.at[:, pl.ds(pl.multiple_of(owner * width, width), width)]

    def shared_block(k, owner):
        return sact.at[owner]

    def remote(source, target, send, receive, device):
        return pltpu.make_async_remote_copy(
            src_ref=source,
            dst_ref=target,
            send_sem=send,
            recv_sem=receive,
            device_id=device,
            device_id_type=MESH,
        )

    def y_copy(view, k, slot, j):
        return remote(view(k, t), view(k, t), y_send.at[slot], y_recv.at[slot], (s, y_peer(j) + c))

    def d_copy(view, k, slot):
        return remote(view(k, t), view(k, t), d_send.at[slot], d_recv.at[slot], (s, partner))

    def f_copy(view, k, slot, j):
        ref = view(k, y_source(j) + c)
        return remote(ref, ref, f_send.at[slot], f_recv.at[slot], (s, partner))

    def spread(view, k, slot):
        for j in range(1, rows_y):
            y_copy(view, k, slot, j).start()
        d_copy(view, k, slot).start()

    def forward(view, k, slot):
        for j in range(1, rows_y):
            y_copy(view, k, slot, j).wait_recv()
        for j in range(1, rows_y):
            f_copy(view, k, slot, j).start()

    def collect(view, k, slot):
        d_copy(view, k, slot).wait_recv()
        for j in range(1, rows_y):
            f_copy(view, k, slot, j).wait_recv()

    def finish_sends(view, k, slot):
        for j in range(1, rows_y):
            y_copy(view, k, slot, j).wait_send()
            f_copy(view, k, slot, j).wait_send()
        d_copy(view, k, slot).wait_send()

    def a_copy(k):
        columns = pl.ds(pl.multiple_of(t * width, width), width)
        relayed = k // half
        source = mate(relayed * half)
        rows = pl.ds(pl.multiple_of(source * cap, cap), cap)
        return remote(
            outgoing.at[k], recv.at[:, rows, columns], a_send.at[k], a_recv.at[k], (mate(k - relayed * half), t)
        )

    def b_copy(k, j):
        rows = pl.ds(pl.multiple_of(s * cap, cap), cap)
        columns = pl.ds(pl.multiple_of((y_source(j) + c) * width, width), width)
        return remote(
            extra.at[k, j - 1], recv.at[:, rows, columns], b_send.at[k, j], b_recv.at[k, j], (mate(k), t)
        )

    def i_copy(k):
        return remote(inverse_out.at[k], inverse_in.at[k], i_send.at[k], i_recv.at[k], (mate(k - k // half * half), t))

    def p_copy(i, source, target):
        return remote(source, target, p_send.at[i], p_recv.at[i], (mate(half), t))

    routes_copy = p_copy(0, routes_rows, far_routes)
    stream_copy = p_copy(1, stream, far_stream)
    inverse_copy = p_copy(2, own_inverse, far_inverse)

    def r_copy(k, e):
        return remote(obuf.at[k, e], ret.at[s, e], r_send.at[k, e], r_recv.at[k, e], (mate(k), t))

    def column_of(row):
        return jnp.broadcast_to(row, (128, row.shape[1])).T[:, 0:1]

    def mixed_block(k, owner):
        return mixed.at[pl.ds(pl.multiple_of(owner * channels, channels), channels), :]

    def edges_block(k, owner):
        return edges.at[owner]

    def sums_block(k, owner):
        return sums.at[owner]

    def gains_block(k, owner):
        return gains.at[owner]

    edge = before.shape[1]
    up_copy = remote(
        product.at[:, pl.ds(tokens_here - edge, edge)], before, h_send.at[0], h_recv.at[0],
        (lax.rem(s + 1, n_sp), t),
    )
    down_copy = remote(
        product.at[:, pl.ds(0, edge)], after, h_send.at[1], h_recv.at[1],
        (lax.rem(s + n_sp - 1, n_sp), t),
    )
    up_copy.start()
    down_copy.start()
    spread(gains_block, 0, GAINS)
    routes_copy.start()

    for load in loads[4:7]:
        load.wait()
    values = product[...].astype(f32)
    place = lax.broadcasted_iota(jnp.int32, (channels, tokens_here), 1)
    tap = taps[...].astype(f32)
    tap_columns = [column_of(tap[j : j + 1]) for j in range(3)]

    def gated(first, last):
        previous = jnp.where(place == 0, first, pltpu.roll(values, 1, 1))
        following = jnp.where(place == tokens_here - 1, last, pltpu.roll(values, tokens_here - 1, 1))
        filtered = tap_columns[0] * previous + tap_columns[1] * values + tap_columns[2] * following
        return (outer[...].astype(f32) * filtered).astype(jnp.bfloat16)

    mixed[pl.ds(pl.multiple_of(t * channels, channels), channels), :] = gated(0.0, 0.0)
    spread(mixed_block, 0, MIXED)

    token_i = lax.broadcasted_iota(jnp.int32, (tokens_here, tokens_here), 0)
    token_j = lax.broadcasted_iota(jnp.int32, (tokens_here, tokens_here), 1)
    choices = routes_rows.shape[0]

    def slots_of(routes):
        one_row = [
            (routes[k : k + 1, :] == lax.broadcasted_iota(jnp.int32, (expert_count, tokens_here), 0)).astype(f32)
            for k in range(choices)
        ]
        earlier_row = jnp.dot(
            sum(one_row).astype(jnp.bfloat16), (token_i < token_j).astype(f32).astype(jnp.bfloat16),
            preferred_element_type=f32,
        )
        rows = [
            routes[k : k + 1, :] * cap + jnp.sum(earlier_row * one_row[k], axis=0, keepdims=True).astype(jnp.int32)
            for k in range(choices)
        ]
        return rows, [column_of(row.astype(f32)).astype(jnp.int32) for row in rows]

    slot_row, slot_column = slots_of(routes_rows[...])

    up_copy.wait_recv()
    down_copy.wait_recv()
    first = jnp.where(s == 0, 0.0, before[...].astype(f32)[:, edge - 1 : edge])
    last = jnp.where(s == n_sp - 1, 0.0, after[...].astype(f32)[:, 0:1])
    complete = gated(first, last).astype(f32)
    left = lax.broadcasted_iota(jnp.int32, (channels, edge), 1) < edge // 2
    edges[t] = jnp.where(left, complete[:, :edge], complete[:, tokens_here - edge :]).astype(jnp.bfloat16)
    spread(edges_block, 0, EDGES)
    forward(mixed_block, 0, MIXED)
    forward(edges_block, 0, EDGES)
    collect(mixed_block, 0, MIXED)
    collect(edges_block, 0, EDGES)
    patched[...] = mixed[...]
    for j in range(n_tp):
        rows = slice(j * channels, (j + 1) * channels)
        border = edges[j].astype(f32)
        start = patched[rows, :edge].astype(f32)
        patched[rows, :edge] = jnp.where(left, border, start).astype(jnp.bfloat16)
        end = patched[rows, tokens_here - edge :].astype(f32)
        patched[rows, tokens_here - edge :] = jnp.where(left, end, border).astype(jnp.bfloat16)
    for load in loads[7:9]:
        load.wait()
    projected = lax.dot_general(
        patched[...], mix[...], (((0,), (0,)), ((), ())), preferred_element_type=f32
    )
    stream[...] = (residual[...].astype(f32) + projected).astype(jnp.bfloat16)
    levels = stream[...].astype(f32)
    own = jnp.broadcast_to(jnp.sum(levels * levels, axis=1, keepdims=True), (tokens_here, 128))
    sums[t] = own.T[:8]
    spread(sums_block, 0, SUMS)
    def picked(peer, slots):
        spot = lax.broadcasted_iota(jnp.int32, (experts * cap, tokens_here), 0) + peer * (experts * cap)
        return sum((spot == slots[k]).astype(f32) for k in range(choices)).astype(jnp.bfloat16)

    def gathered(chosen, columns):
        return jnp.dot(chosen, columns, preferred_element_type=f32).astype(jnp.bfloat16)

    def pack(k, peer, slots, values):
        packed = gathered(picked(peer, slots), values)
        for e in range(experts):
            outgoing[k, e] = packed[e * cap : (e + 1) * cap]
        a_copy(k).start()

    stream_copy.start()
    own_whole = pltpu.make_async_copy(stream, whole_block(0, t), own_sem)
    own_whole.start()
    own_whole.wait()
    spread(whole_block, 0, WHOLE)

    @pl.loop(1, half)
    def _(k):
        pack(k, mate(k), slot_row, stream[...])

    routes_copy.wait_recv()
    far_row, far_column = slots_of(far_routes[...])
    forward(gains_block, 0, GAINS)
    forward(sums_block, 0, SUMS)
    collect(gains_block, 0, GAINS)
    for j in range(n_tp):
        gain_row[:, j * width : (j + 1) * width] = gains[j]
    collect(sums_block, 0, SUMS)
    squares = sums[0]
    for j in range(1, n_tp):
        squares = squares + sums[j]
    inverse_row = lax.rsqrt(squares[0:1] / D + epsilon)
    own_inverse[...] = jnp.broadcast_to(inverse_row, own_inverse.shape)
    inverse_copy.start()
    inverse_rms = column_of(inverse_row)

    def inverses(peer, slots, values):
        spot = lax.broadcasted_iota(jnp.int32, (tokens_here, inverse_in.shape[2]), 1) + peer * (experts * cap)
        hits = sum(jnp.where(spot == slots[k], values, 0.0) for k in range(choices))
        return jnp.broadcast_to(jnp.sum(hits, axis=0, keepdims=True), inverse_in.shape[1:])

    inverse_in[0] = inverses(s, slot_column, inverse_rms)

    @pl.loop(1, half)
    def _(k):
        inverse_out[k] = inverses(mate(k), slot_column, inverse_rms)
        i_copy(k).start()

    def arrive(i):
        k = chunk(i)
        a_copy(k).wait_recv()

        @pl.when(jnp.logical_not(whole_rows(k)))
        def _():
            spread(block, k, DISPATCH + k)

        @pl.when(whole_rows(k))
        def _():
            for j in range(1, rows_y):
                b_copy(k, j).wait_recv()
            d_copy(block, k, DISPATCH + k).start()
            for j in range(1, rows_y):
                f_copy(block, k, DISPATCH + k, j).start()

    def pass_on(i):
        k = chunk(i)

        @pl.when(jnp.logical_not(whole_rows(k)))
        def _():
            forward(block, k, DISPATCH + k)

    arrive(1)
    forward(whole_block, 0, WHOLE)
    collect(whole_block, 0, WHOLE)

    def expert_in(k):
        rows = rows_of(k)
        columns = pl.ds(pl.multiple_of(t * hidden_width, hidden_width), hidden_width)
        inverse = column_of(inverse_in[k][0:1])
        for e in range(experts):
            x = recv[e, rows, :].astype(f32) * inverse[e * cap : (e + 1) * cap] * gain_row[0:1]
            x = x.astype(jnp.bfloat16)
            gate = jnp.dot(x, gate_w[e], preferred_element_type=jnp.float32)
            up = jnp.dot(x, up_w[e], preferred_element_type=jnp.float32)
            hid[e, rows, columns] = (jax.nn.silu(gate) * up).astype(jnp.bfloat16)
            spread(hidden_block(e), k, HIDDEN + k * experts + e)

    own_rows = gathered(picked(s, slot_row), whole[...])
    for e in range(experts):
        recv[e, rows_of(0), :] = own_rows[e * cap : (e + 1) * cap]
    for load in loads[9:]:
        load.wait()
    expert_in(0)

    def pack_extra(k):
        chosen = picked(mate(k), slot_row)
        for j in range(1, rows_y):
            columns = pl.ds(pl.multiple_of((y_source(j) + c) * width, width), width)
            packed = gathered(chosen, whole[:, columns])
            for e in range(experts):
                extra[k, j - 1, e] = packed[e * cap : (e + 1) * cap]
            b_copy(k, j).start()

    def take(i):
        k = chunk(i)
        pass_on(i)

        @pl.when(k != half)
        def _():
            i_copy(k).wait_recv()

        collect(block, k, DISPATCH + k)
        expert_in(k)

    take(1)
    stream_copy.wait_recv()

    @pl.loop(half + 1, n_sp)
    def _(k):
        pack(k, mate(k - half), far_row, far_stream[...])

    far_rows = gathered(picked(s, far_row), far_stream[...])
    for e in range(experts):
        recv[e, rows_of(half), pl.ds(pl.multiple_of(t * width, width), width)] = far_rows[e * cap : (e + 1) * cap]
    spread(block, half, DISPATCH + half)
    @pl.loop(2, near)
    def _(k):
        pack_extra(k)

    normed[...] = (whole[...].astype(f32) * inverse_rms * gain_row[0:1]).astype(jnp.bfloat16)
    tokens = normed[...]
    shared_hidden = jax.nn.silu(jnp.dot(tokens, sgate[...], preferred_element_type=jnp.float32)) * jnp.dot(
        tokens, sup[...], preferred_element_type=jnp.float32
    )
    sact[t] = shared_hidden.astype(jnp.bfloat16)
    spread(shared_block, 0, SHARED)

    inverse_copy.wait_recv()
    far_rms = column_of(far_inverse[0:1])
    inverse_in[half] = inverses(s, far_column, far_rms)

    @pl.loop(half + 1, n_sp)
    def _(k):
        inverse_out[k] = inverses(mate(k - half), far_column, far_rms)
        i_copy(k).start()

    weight_rows = scores[...] / jnp.sum(scores[...], axis=0, keepdims=True) * routed_scale
    weights = [column_of(weight_rows[k : k + 1]) for k in range(choices)]

    def returned(k):
        group = mate(k)
        spot = lax.broadcasted_iota(jnp.int32, (tokens_here, experts * cap), 1) + group * (experts * cap)
        rows = ret[group].reshape(experts * cap, width)
        total = shared_out[...]
        for j in range(choices):
            chosen = (spot == slot_column[j]).astype(f32).astype(jnp.bfloat16)
            total = total + weights[j] * jnp.dot(chosen, rows, preferred_element_type=f32)
        return total

    @pl.loop(2, n_sp + 6)
    def _(i):
        @pl.when((i > 2) & (i < n_sp))
        def _():
            arrive(i)

        early = jnp.where(i >= n_sp - 1, 1, 0)
        ahead = jnp.where(i >= n_sp - 2, 1, 0)

        @pl.when((i > 2) & (i < n_sp))
        def _():
            @pl.loop(i - 1 + early, i + ahead)
            def _(p):
                take(p)

        @pl.when(i < n_sp + 2)
        def _():
            k = chunk(i - 2)
            rows = rows_of(k)
            for e in range(experts):
                forward(hidden_block(e), k, HIDDEN + k * experts + e)
                collect(hidden_block(e), k, HIDDEN + k * experts + e)
                obuf[k, e] = jnp.dot(
                    hid[e, rows, :], down_w[e], preferred_element_type=jnp.float32
                ).astype(jnp.bfloat16)

                @pl.when(k > 0)
                def _():
                    r_copy(k, e).start()

            @pl.when(k == 0)
            def _():
                ret[s] = obuf[0]

        @pl.when(i == 3)
        def _():
            forward(shared_block, 0, SHARED)

        @pl.when(i == 4)
        def _():
            collect(shared_block, 0, SHARED)
            total = jnp.zeros(shared_out.shape, jnp.float32)
            for j in range(n_tp):
                rows = sdown[pl.ds(j * shared_width, shared_width), :]
                total = total + jnp.dot(sact[j], rows, preferred_element_type=jnp.float32)
            shared_out[...] = total

        @pl.when(i >= 7)
        def _():
            k = entry(combine, i - 7)

            @pl.when(k > 0)
            def _():
                for e in range(experts):
                    r_copy(k, e).wait_recv()

            shared_out[...] = returned(k)

    routes_copy.wait_send()
    stream_copy.wait_send()
    inverse_copy.wait_send()
    up_copy.wait_send()
    down_copy.wait_send()
    finish_sends(mixed_block, 0, MIXED)
    finish_sends(edges_block, 0, EDGES)
    finish_sends(sums_block, 0, SUMS)
    finish_sends(gains_block, 0, GAINS)
    finish_sends(whole_block, 0, WHOLE)
    finish_sends(shared_block, 0, SHARED)

    for e in range(experts):
        finish_sends(hidden_block(e), 0, HIDDEN + e)

    @pl.loop(1, n_sp)
    def _(k):
        for e in range(experts):
            finish_sends(hidden_block(e), k, HIDDEN + k * experts + e)
            r_copy(k, e).wait_send()

        @pl.when(k != half)
        def _():
            a_copy(k).wait_send()
            i_copy(k).wait_send()

        @pl.when(jnp.logical_not(whole_rows(k)))
        def _():
            finish_sends(block, k, DISPATCH + k)

        @pl.when(whole_rows(k))
        def _():
            d_copy(block, k, DISPATCH + k).wait_send()
            for j in range(1, rows_y):
                f_copy(block, k, DISPATCH + k, j).wait_send()
                b_copy(k, j).wait_send()

    for e in range(experts):
        r_copy(combine[-1], e).wait_recv()
    out[...] = (stream[...].astype(f32) + returned(combine[-1])).astype(jnp.bfloat16)


def local(
    outer_gate,
    inner_gate,
    conv_input,
    conv_taps,
    mix_weight,
    residual,
    norm_gain,
    routes,
    route_scores,
    expert_gate,
    expert_up,
    expert_down,
    shared_gate,
    shared_up,
    shared_down,
):
    n_sp, n_tp = lax.axis_size("sp"), lax.axis_size("tp")
    experts, depth, hidden_width = expert_gate.shape
    channels, token_count = outer_gate.shape
    width = residual.shape[1]
    cap = 2 * token_count * routes.shape[1] // (experts * n_sp)
    cap = (cap + 15) // 16 * 16
    slots = n_sp * (1 + experts) + 6
    edge = min(128, token_count)
    lanes = (experts * cap + 127) // 128 * 128
    vmem = pl.BlockSpec(memory_space=pltpu.VMEM)
    hbm = pl.BlockSpec(memory_space=pltpu.HBM)
    bf16 = jnp.bfloat16
    dma = pltpu.SemaphoreType.DMA
    return pl.pallas_call(
        functools.partial(moe_kernel, n_sp, n_tp),
        name="moe",
        out_shape=pltpu.VMEM((token_count, width), bf16),
        in_specs=[hbm] * 15,
        out_specs=vmem,
        scratch_shapes=[
            pltpu.VMEM((n_sp, experts, cap, width), bf16),
            pltpu.VMEM((token_count, width), jnp.float32),
            pltpu.VMEM((n_sp, experts, cap, width), bf16),
            pltpu.VMEM((n_sp // 2, n_tp // 2 - 1, experts, cap, width), bf16),
            pltpu.VMEM((token_count, width * n_tp), bf16),
            pltpu.VMEM((token_count, width), bf16),
            pltpu.VMEM((channels, token_count), bf16),
            pltpu.VMEM((channels, edge), bf16),
            pltpu.VMEM((channels, edge), bf16),
            pltpu.VMEM((channels * n_tp, token_count), bf16),
            pltpu.VMEM((n_tp, channels, edge), bf16),
            pltpu.VMEM((channels * n_tp, token_count), bf16),
            pltpu.VMEM((n_tp, 8, token_count), jnp.float32),
            pltpu.VMEM((n_tp, 8, width), jnp.float32),
            pltpu.VMEM((8, width * n_tp), jnp.float32),
            pltpu.VMEM((n_sp, 8, lanes), jnp.float32),
            pltpu.VMEM((n_sp, 8, lanes), jnp.float32),
            pltpu.VMEM((8, token_count), jnp.float32),
            pltpu.VMEM((8, token_count), jnp.float32),
            pltpu.VMEM((routes.shape[1], token_count), jnp.int32),
            pltpu.VMEM((token_count, width), bf16),
            pltpu.VMEM((experts, n_sp * cap, width * n_tp), bf16),
            pltpu.VMEM((experts, n_sp * cap, hidden_width * n_tp), bf16),
            pltpu.VMEM((token_count, width * n_tp), bf16),
            pltpu.VMEM((n_tp, token_count, shared_gate.shape[1]), bf16),
            pltpu.VMEM((n_sp, experts, cap, width), bf16),
            pltpu.VMEM(outer_gate.shape, bf16),
            pltpu.VMEM(inner_gate.shape, bf16),
            pltpu.VMEM(conv_input.shape, bf16),
            pltpu.VMEM(conv_taps.shape, bf16),
            pltpu.VMEM(norm_gain.shape, bf16),
            pltpu.VMEM(routes.shape[::-1], jnp.int32),
            pltpu.VMEM(route_scores.shape[::-1], jnp.float32),
            pltpu.VMEM(mix_weight.shape, bf16),
            pltpu.VMEM(residual.shape, bf16),
            pltpu.VMEM(expert_gate.shape, bf16),
            pltpu.VMEM(expert_up.shape, bf16),
            pltpu.VMEM(expert_down.shape, bf16),
            pltpu.VMEM(shared_gate.shape, bf16),
            pltpu.VMEM(shared_up.shape, bf16),
            pltpu.VMEM(shared_down.shape, bf16),
            dma((15,)),
            dma,
            dma((2,)),
            dma((2,)),
            dma((n_sp,)),
            dma((n_sp,)),
            dma((n_sp // 2, n_tp // 2)),
            dma((n_sp // 2, n_tp // 2)),
            dma((n_sp,)),
            dma((n_sp,)),
            dma((3,)),
            dma((3,)),
            dma((slots,)),
            dma((slots,)),
            dma((slots,)),
            dma((slots,)),
            dma((slots,)),
            dma((slots,)),
            dma((n_sp, experts)),
            dma((n_sp, experts)),
        ],
        compiler_params=pltpu.CompilerParams(
            collective_id=0, has_side_effects=True, vmem_limit_bytes=VMEM_LIMIT
        ),
    )(
        outer_gate,
        inner_gate,
        conv_input,
        conv_taps,
        norm_gain,
        routes.T,
        route_scores.T,
        mix_weight,
        residual,
        expert_gate,
        expert_up,
        expert_down,
        shared_gate,
        shared_up,
        shared_down,
    )


def solution(mesh):
    in_specs = (
        P("tp", "sp"),
        P("tp", "sp"),
        P("tp", "sp"),
        P(None, "tp"),
        P(None, "tp"),
        P("sp", "tp"),
        P("tp"),
        P("sp", None),
        P("sp", None),
        P("sp", None, "tp"),
        P("sp", None, "tp"),
        P("sp", None, "tp"),
        P(None, "tp"),
        P(None, "tp"),
        P(None, "tp"),
    )
    out_specs = P("sp", "tp")
    return jax.shard_map(local, mesh=mesh, in_specs=in_specs, out_specs=out_specs, check_vma=False)
```

```python
import functools

import jax
import jax.numpy as jnp
from jax import lax
from jax.experimental import pallas as pl
from jax.experimental.pallas import tpu as pltpu
from jax.sharding import PartitionSpec as P

D = 2048


epsilon = 1e-06
routed_scale = 2.5


MESH = pl.DeviceIdType.MESH
VMEM_LIMIT = 58 * 2**20


def moe_kernel(
    n_sp,
    n_tp,
    outer_hbm,
    inner_hbm,
    conv_hbm,
    taps_hbm,
    gain_hbm,
    routes_hbm,
    scores_hbm,
    mix_hbm,
    residual_hbm,
    gate_hbm,
    up_hbm,
    down_hbm,
    sgate_hbm,
    sup_hbm,
    sdown_hbm,
    out,
    ret,
    shared_out,
    outgoing,
    extra,
    normed,
    stream,
    product,
    before,
    after,
    mixed,
    edges,
    patched,
    sums,
    gains,
    gain_row,
    inverse_out,
    inverse_in,
    own_inverse,
    far_inverse,
    far_routes,
    far_stream,
    recv,
    hid,
    whole,
    sact,
    obuf,
    outer,
    inner,
    conv,
    taps,
    gain,
    routes_rows,
    scores,
    mix,
    residual,
    gate_w,
    up_w,
    down_w,
    sgate,
    sup,
    sdown,
    load_sem,
    h_send,
    h_recv,
    a_send,
    a_recv,
    b_send,
    b_recv,
    i_send,
    i_recv,
    p_send,
    p_recv,
    y_send,
    y_recv,
    d_send,
    d_recv,
    f_send,
    f_recv,
    r_send,
    r_recv,
):
    s = lax.axis_index("sp")
    t = lax.axis_index("tp")
    rows_y = n_tp // 2
    y, c = t // 2, lax.rem(t, 2)
    partner = y * 2 + (1 - c)
    experts, cap, width = outgoing.shape[1:]
    hidden_width = gate_w.shape[2]
    shared_width = sgate.shape[1]
    DISPATCH, HIDDEN = 0, n_sp
    WHOLE, SHARED, MIXED, SUMS, GAINS, EDGES = (n_sp * (1 + experts) + j for j in range(6))
    channels, tokens_here = outer.shape
    expert_count = n_sp * experts
    f32 = jnp.float32

    half = n_sp // 2
    near = half if rows_y == 2 else 2
    quarter = half // 2
    central = lax.rem((s // quarter + 1) // 2, 2)
    order = [1, half, *range(2, half), *range(half + 1, n_sp)]
    outer_order = order
    combine = [0, *order]
    if near > 2:
        late = list(range(half + 2, n_sp))
        nearest = list(range(2, near))
        order = [1, half, half + 1, *late, *nearest]
        outer_order = [1, half, *late, half + 1, *nearest]
        combine = [0, 1, half, late[0], half + 1, *late[1:], *nearest]

    def whole_rows(k):
        return (k > 1) & (k < near)

    def entry(table, i):
        return sum(jnp.where(i == p, k, 0) for p, k in enumerate(table))

    def chunk(i):
        return central * entry([0, *order], i) + (1 - central) * entry([0, *outer_order], i)

    def mate(k):
        total, bit = 0, 1
        while bit < n_sp:
            total = total + lax.rem(s // bit + k // bit, 2) * bit
            bit *= 2
        return total

    def y_peer(j):
        return lax.rem(y + j, rows_y) * 2

    def y_source(j):
        return lax.rem(y - j + rows_y, rows_y) * 2

    barrier = pltpu.get_barrier_semaphore()
    for j in range(1, n_sp):
        pl.semaphore_signal(barrier, inc=1, device_id=(mate(j), t), device_id_type=MESH)
    for j in range(1, rows_y):
        pl.semaphore_signal(barrier, inc=1, device_id=(s, y_peer(j) + c), device_id_type=MESH)
    pl.semaphore_signal(barrier, inc=1, device_id=(s, partner), device_id_type=MESH)

    places = (
        (inner_hbm, inner),
        (conv_hbm, conv),
        (gain_hbm, gain),
        (routes_hbm, routes_rows),
        (outer_hbm, outer),
        (taps_hbm, taps),
        (scores_hbm, scores),
        (mix_hbm, mix),
        (residual_hbm, residual),
        (gate_hbm, gate_w),
        (up_hbm, up_w),
        (down_hbm, down_w),
        (sgate_hbm, sgate),
        (sup_hbm, sup),
        (sdown_hbm, sdown),
    )
    loads = [pltpu.make_async_copy(source, target, load_sem.at[i]) for i, (source, target) in enumerate(places)]
    for load in loads:
        load.start()
    for load in loads[:4]:
        load.wait()
    filtered_input = inner[...].astype(f32) * conv[...].astype(f32)
    product[...] = filtered_input.astype(jnp.bfloat16)
    gains[t] = jnp.broadcast_to(gain[...].astype(f32).reshape(1, width), gains.shape[1:])
    pl.semaphore_wait(barrier, n_sp - 1 + rows_y - 1 + 1)

    def rows_of(k):
        return pl.ds(pl.multiple_of(mate(k) * cap, cap), cap)

    def block(k, owner):
        return recv.at[:, rows_of(k), pl.ds(pl.multiple_of(owner * width, width), width)]

    def hidden_block(e):
        def view(k, owner):
            columns = pl.ds(pl.multiple_of(owner * hidden_width, hidden_width), hidden_width)
            return hid.at[e, rows_of(k), columns]

        return view

    def whole_block(k, owner):
        return whole.at[:, pl.ds(pl.multiple_of(owner * width, width), width)]

    def shared_block(k, owner):
        return sact.at[owner]

    def remote(source, target, send, receive, device):
        return pltpu.make_async_remote_copy(
            src_ref=source,
            dst_ref=target,
            send_sem=send,
            recv_sem=receive,
            device_id=device,
            device_id_type=MESH,
        )

    def y_copy(view, k, slot, j):
        return remote(view(k, t), view(k, t), y_send.at[slot], y_recv.at[slot], (s, y_peer(j) + c))

    def d_copy(view, k, slot):
        return remote(view(k, t), view(k, t), d_send.at[slot], d_recv.at[slot], (s, partner))

    def f_copy(view, k, slot, j):
        ref = view(k, y_source(j) + c)
        return remote(ref, ref, f_send.at[slot], f_recv.at[slot], (s, partner))

    def spread(view, k, slot):
        for j in range(1, rows_y):
            y_copy(view, k, slot, j).start()
        d_copy(view, k, slot).start()

    def forward(view, k, slot):
        for j in range(1, rows_y):
            y_copy(view, k, slot, j).wait_recv()
        for j in range(1, rows_y):
            f_copy(view, k, slot, j).start()

    def collect(view, k, slot):
        d_copy(view, k, slot).wait_recv()
        for j in range(1, rows_y):
            f_copy(view, k, slot, j).wait_recv()

    def finish_sends(view, k, slot):
        for j in range(1, rows_y):
            y_copy(view, k, slot, j).wait_send()
            f_copy(view, k, slot, j).wait_send()
        d_copy(view, k, slot).wait_send()

    def a_copy(k):
        columns = pl.ds(pl.multiple_of(t * width, width), width)
        relayed = k // half
        source = mate(relayed * half)
        rows = pl.ds(pl.multiple_of(source * cap, cap), cap)
        return remote(
            outgoing.at[k], recv.at[:, rows, columns], a_send.at[k], a_recv.at[k], (mate(k - relayed * half), t)
        )

    def b_copy(k, j):
        rows = pl.ds(pl.multiple_of(s * cap, cap), cap)
        columns = pl.ds(pl.multiple_of((y_source(j) + c) * width, width), width)
        return remote(
            extra.at[k, j - 1], recv.at[:, rows, columns], b_send.at[k, j], b_recv.at[k, j], (mate(k), t)
        )

    def i_copy(k):
        return remote(inverse_out.at[k], inverse_in.at[k], i_send.at[k], i_recv.at[k], (mate(k - k // half * half), t))

    def p_copy(i, source, target):
        return remote(source, target, p_send.at[i], p_recv.at[i], (mate(half), t))

    routes_copy = p_copy(0, routes_rows, far_routes)
    stream_copy = p_copy(1, stream, far_stream)
    inverse_copy = p_copy(2, own_inverse, far_inverse)

    def r_copy(k, e):
        return remote(obuf.at[k, e], ret.at[s, e], r_send.at[k, e], r_recv.at[k, e], (mate(k), t))

    def column_of(row):
        return jnp.broadcast_to(row, (128, row.shape[1])).T[:, 0:1]

    def mixed_block(k, owner):
        return mixed.at[pl.ds(pl.multiple_of(owner * channels, channels), channels), :]

    def edges_block(k, owner):
        return edges.at[owner]

    def sums_block(k, owner):
        return sums.at[owner]

    def gains_block(k, owner):
        return gains.at[owner]

    edge = before.shape[1]
    up_copy = remote(
        product.at[:, pl.ds(tokens_here - edge, edge)], before, h_send.at[0], h_recv.at[0],
        (lax.rem(s + 1, n_sp), t),
    )
    down_copy = remote(
        product.at[:, pl.ds(0, edge)], after, h_send.at[1], h_recv.at[1],
        (lax.rem(s + n_sp - 1, n_sp), t),
    )
    up_copy.start()
    down_copy.start()
    spread(gains_block, 0, GAINS)
    routes_copy.start()

    for load in loads[4:7]:
        load.wait()
    values = product[...].astype(f32)
    place = lax.broadcasted_iota(jnp.int32, (channels, tokens_here), 1)
    tap = taps[...].astype(f32)
    tap_columns = [column_of(tap[j : j + 1]) for j in range(3)]

    def gated(first, last):
        previous = jnp.where(place == 0, first, pltpu.roll(values, 1, 1))
        following = jnp.where(place == tokens_here - 1, last, pltpu.roll(values, tokens_here - 1, 1))
        filtered = tap_columns[0] * previous + tap_columns[1] * values + tap_columns[2] * following
        return (outer[...].astype(f32) * filtered).astype(jnp.bfloat16)

    mixed[pl.ds(pl.multiple_of(t * channels, channels), channels), :] = gated(0.0, 0.0)
    spread(mixed_block, 0, MIXED)

    token_i = lax.broadcasted_iota(jnp.int32, (tokens_here, tokens_here), 0)
    token_j = lax.broadcasted_iota(jnp.int32, (tokens_here, tokens_here), 1)
    choices = routes_rows.shape[0]

    def slots_of(routes):
        one_row = [
            (routes[k : k + 1, :] == lax.broadcasted_iota(jnp.int32, (expert_count, tokens_here), 0)).astype(f32)
            for k in range(choices)
        ]
        earlier_row = jnp.dot(
            sum(one_row).astype(jnp.bfloat16), (token_i < token_j).astype(f32).astype(jnp.bfloat16),
            preferred_element_type=f32,
        )
        rows = [
            routes[k : k + 1, :] * cap + jnp.sum(earlier_row * one_row[k], axis=0, keepdims=True).astype(jnp.int32)
            for k in range(choices)
        ]
        return rows, [column_of(row.astype(f32)).astype(jnp.int32) for row in rows]

    slot_row, slot_column = slots_of(routes_rows[...])

    up_copy.wait_recv()
    down_copy.wait_recv()
    first = jnp.where(s == 0, 0.0, before[...].astype(f32)[:, edge - 1 : edge])
    last = jnp.where(s == n_sp - 1, 0.0, after[...].astype(f32)[:, 0:1])
    complete = gated(first, last).astype(f32)
    left = lax.broadcasted_iota(jnp.int32, (channels, edge), 1) < edge // 2
    edges[t] = jnp.where(left, complete[:, :edge], complete[:, tokens_here - edge :]).astype(jnp.bfloat16)
    spread(edges_block, 0, EDGES)
    forward(mixed_block, 0, MIXED)
    forward(edges_block, 0, EDGES)
    collect(mixed_block, 0, MIXED)
    collect(edges_block, 0, EDGES)
    patched[...] = mixed[...]
    for j in range(n_tp):
        rows = slice(j * channels, (j + 1) * channels)
        border = edges[j].astype(f32)
        start = patched[rows, :edge].astype(f32)
        patched[rows, :edge] = jnp.where(left, border, start).astype(jnp.bfloat16)
        end = patched[rows, tokens_here - edge :].astype(f32)
        patched[rows, tokens_here - edge :] = jnp.where(left, end, border).astype(jnp.bfloat16)
    for load in loads[7:9]:
        load.wait()
    projected = lax.dot_general(
        patched[...], mix[...], (((0,), (0,)), ((), ())), preferred_element_type=f32
    )
    stream[...] = (residual[...].astype(f32) + projected).astype(jnp.bfloat16)
    levels = stream[...].astype(f32)
    own = jnp.broadcast_to(jnp.sum(levels * levels, axis=1, keepdims=True), (tokens_here, 128))
    sums[t] = own.T[:8]
    spread(sums_block, 0, SUMS)
    def picked(peer, slots):
        spot = lax.broadcasted_iota(jnp.int32, (experts * cap, tokens_here), 0) + peer * (experts * cap)
        return sum((spot == slots[k]).astype(f32) for k in range(choices)).astype(jnp.bfloat16)

    def gathered(chosen, columns):
        return jnp.dot(chosen, columns, preferred_element_type=f32).astype(jnp.bfloat16)

    def pack(k, peer, slots, values):
        packed = gathered(picked(peer, slots), values)
        for e in range(experts):
            outgoing[k, e] = packed[e * cap : (e + 1) * cap]
        a_copy(k).start()

    whole[:, pl.ds(pl.multiple_of(t * width, width), width)] = stream[...]
    spread(whole_block, 0, WHOLE)
    stream_copy.start()

    @pl.loop(1, half)
    def _(k):
        pack(k, mate(k), slot_row, stream[...])

    routes_copy.wait_recv()
    far_row, far_column = slots_of(far_routes[...])
    forward(gains_block, 0, GAINS)
    forward(sums_block, 0, SUMS)
    collect(gains_block, 0, GAINS)
    for j in range(n_tp):
        gain_row[:, j * width : (j + 1) * width] = gains[j]
    collect(sums_block, 0, SUMS)
    squares = sums[0]
    for j in range(1, n_tp):
        squares = squares + sums[j]
    inverse_row = lax.rsqrt(squares[0:1] / D + epsilon)
    own_inverse[...] = jnp.broadcast_to(inverse_row, own_inverse.shape)
    inverse_copy.start()
    inverse_rms = column_of(inverse_row)

    def inverses(peer, slots, values):
        spot = lax.broadcasted_iota(jnp.int32, (tokens_here, inverse_in.shape[2]), 1) + peer * (experts * cap)
        hits = sum(jnp.where(spot == slots[k], values, 0.0) for k in range(choices))
        return jnp.broadcast_to(jnp.sum(hits, axis=0, keepdims=True), inverse_in.shape[1:])

    inverse_in[0] = inverses(s, slot_column, inverse_rms)

    @pl.loop(1, half)
    def _(k):
        inverse_out[k] = inverses(mate(k), slot_column, inverse_rms)
        i_copy(k).start()

    def arrive(i):
        k = chunk(i)
        a_copy(k).wait_recv()

        @pl.when(jnp.logical_not(whole_rows(k)))
        def _():
            spread(block, k, DISPATCH + k)

        @pl.when(whole_rows(k))
        def _():
            for j in range(1, rows_y):
                b_copy(k, j).wait_recv()
            d_copy(block, k, DISPATCH + k).start()
            for j in range(1, rows_y):
                f_copy(block, k, DISPATCH + k, j).start()

    def pass_on(i):
        k = chunk(i)

        @pl.when(jnp.logical_not(whole_rows(k)))
        def _():
            forward(block, k, DISPATCH + k)

    arrive(1)
    forward(whole_block, 0, WHOLE)
    collect(whole_block, 0, WHOLE)

    def expert_in(k):
        rows = rows_of(k)
        columns = pl.ds(pl.multiple_of(t * hidden_width, hidden_width), hidden_width)
        inverse = column_of(inverse_in[k][0:1])
        for e in range(experts):
            x = recv[e, rows, :].astype(f32) * inverse[e * cap : (e + 1) * cap] * gain_row[0:1]
            x = x.astype(jnp.bfloat16)
            gate = jnp.dot(x, gate_w[e], preferred_element_type=jnp.float32)
            up = jnp.dot(x, up_w[e], preferred_element_type=jnp.float32)
            hid[e, rows, columns] = (jax.nn.silu(gate) * up).astype(jnp.bfloat16)
            spread(hidden_block(e), k, HIDDEN + k * experts + e)

    own_rows = gathered(picked(s, slot_row), whole[...])
    for e in range(experts):
        recv[e, rows_of(0), :] = own_rows[e * cap : (e + 1) * cap]
    for load in loads[9:]:
        load.wait()
    expert_in(0)

    def pack_extra(k):
        chosen = picked(mate(k), slot_row)
        for j in range(1, rows_y):
            columns = pl.ds(pl.multiple_of((y_source(j) + c) * width, width), width)
            packed = gathered(chosen, whole[:, columns])
            for e in range(experts):
                extra[k, j - 1, e] = packed[e * cap : (e + 1) * cap]
            b_copy(k, j).start()

    def take(i):
        k = chunk(i)
        pass_on(i)

        @pl.when(k != half)
        def _():
            i_copy(k).wait_recv()

        collect(block, k, DISPATCH + k)
        expert_in(k)

    take(1)
    stream_copy.wait_recv()

    @pl.loop(half + 1, n_sp)
    def _(k):
        pack(k, mate(k - half), far_row, far_stream[...])

    far_rows = gathered(picked(s, far_row), far_stream[...])
    for e in range(experts):
        recv[e, rows_of(half), pl.ds(pl.multiple_of(t * width, width), width)] = far_rows[e * cap : (e + 1) * cap]
    spread(block, half, DISPATCH + half)
    normed[...] = (whole[...].astype(f32) * inverse_rms * gain_row[0:1]).astype(jnp.bfloat16)
    tokens = normed[...]
    shared_hidden = jax.nn.silu(jnp.dot(tokens, sgate[...], preferred_element_type=jnp.float32)) * jnp.dot(
        tokens, sup[...], preferred_element_type=jnp.float32
    )
    sact[t] = shared_hidden.astype(jnp.bfloat16)
    spread(shared_block, 0, SHARED)

    inverse_copy.wait_recv()
    far_rms = column_of(far_inverse[0:1])
    inverse_in[half] = inverses(s, far_column, far_rms)

    @pl.loop(half + 1, n_sp)
    def _(k):
        inverse_out[k] = inverses(mate(k - half), far_column, far_rms)
        i_copy(k).start()

    @pl.loop(2, near)
    def _(k):
        pack_extra(k)

    weight_rows = scores[...] / jnp.sum(scores[...], axis=0, keepdims=True) * routed_scale
    weights = [column_of(weight_rows[k : k + 1]) for k in range(choices)]

    def returned(k):
        group = mate(k)
        spot = lax.broadcasted_iota(jnp.int32, (tokens_here, experts * cap), 1) + group * (experts * cap)
        rows = ret[group].reshape(experts * cap, width)
        total = shared_out[...]
        for j in range(choices):
            chosen = (spot == slot_column[j]).astype(f32).astype(jnp.bfloat16)
            total = total + weights[j] * jnp.dot(chosen, rows, preferred_element_type=f32)
        return total

    @pl.loop(2, n_sp + 6)
    def _(i):
        @pl.when((i > 2) & (i < n_sp))
        def _():
            arrive(i)

        early = jnp.where(i >= n_sp - 1, 1, 0)
        ahead = jnp.where(i >= n_sp - 2, 1, 0)

        @pl.when((i > 2) & (i < n_sp))
        def _():
            @pl.loop(i - 1 + early, i + ahead)
            def _(p):
                take(p)

        @pl.when(i < n_sp + 2)
        def _():
            k = chunk(i - 2)
            rows = rows_of(k)
            for e in range(experts):
                forward(hidden_block(e), k, HIDDEN + k * experts + e)
                collect(hidden_block(e), k, HIDDEN + k * experts + e)
                obuf[k, e] = jnp.dot(
                    hid[e, rows, :], down_w[e], preferred_element_type=jnp.float32
                ).astype(jnp.bfloat16)

                @pl.when(k > 0)
                def _():
                    r_copy(k, e).start()

            @pl.when(k == 0)
            def _():
                ret[s] = obuf[0]

        @pl.when(i == 3)
        def _():
            forward(shared_block, 0, SHARED)

        @pl.when(i == 4)
        def _():
            collect(shared_block, 0, SHARED)
            total = jnp.zeros(shared_out.shape, jnp.float32)
            for j in range(n_tp):
                rows = sdown[pl.ds(j * shared_width, shared_width), :]
                total = total + jnp.dot(sact[j], rows, preferred_element_type=jnp.float32)
            shared_out[...] = total

        @pl.when(i >= 7)
        def _():
            k = entry(combine, i - 7)

            @pl.when(k > 0)
            def _():
                for e in range(experts):
                    r_copy(k, e).wait_recv()

            shared_out[...] = returned(k)

    routes_copy.wait_send()
    stream_copy.wait_send()
    inverse_copy.wait_send()
    up_copy.wait_send()
    down_copy.wait_send()
    finish_sends(mixed_block, 0, MIXED)
    finish_sends(edges_block, 0, EDGES)
    finish_sends(sums_block, 0, SUMS)
    finish_sends(gains_block, 0, GAINS)
    finish_sends(whole_block, 0, WHOLE)
    finish_sends(shared_block, 0, SHARED)

    for e in range(experts):
        finish_sends(hidden_block(e), 0, HIDDEN + e)

    @pl.loop(1, n_sp)
    def _(k):
        for e in range(experts):
            finish_sends(hidden_block(e), k, HIDDEN + k * experts + e)
            r_copy(k, e).wait_send()

        @pl.when(k != half)
        def _():
            a_copy(k).wait_send()
            i_copy(k).wait_send()

        @pl.when(jnp.logical_not(whole_rows(k)))
        def _():
            finish_sends(block, k, DISPATCH + k)

        @pl.when(whole_rows(k))
        def _():
            d_copy(block, k, DISPATCH + k).wait_send()
            for j in range(1, rows_y):
                f_copy(block, k, DISPATCH + k, j).wait_send()
                b_copy(k, j).wait_send()

    for e in range(experts):
        r_copy(combine[-1], e).wait_recv()
    out[...] = (stream[...].astype(f32) + returned(combine[-1])).astype(jnp.bfloat16)


def local(
    outer_gate,
    inner_gate,
    conv_input,
    conv_taps,
    mix_weight,
    residual,
    norm_gain,
    routes,
    route_scores,
    expert_gate,
    expert_up,
    expert_down,
    shared_gate,
    shared_up,
    shared_down,
):
    n_sp, n_tp = lax.axis_size("sp"), lax.axis_size("tp")
    experts, depth, hidden_width = expert_gate.shape
    channels, token_count = outer_gate.shape
    width = residual.shape[1]
    cap = 2 * token_count * routes.shape[1] // (experts * n_sp)
    cap = (cap + 15) // 16 * 16
    slots = n_sp * (1 + experts) + 6
    edge = min(128, token_count)
    lanes = (experts * cap + 127) // 128 * 128
    vmem = pl.BlockSpec(memory_space=pltpu.VMEM)
    hbm = pl.BlockSpec(memory_space=pltpu.HBM)
    bf16 = jnp.bfloat16
    dma = pltpu.SemaphoreType.DMA
    return pl.pallas_call(
        functools.partial(moe_kernel, n_sp, n_tp),
        name="moe",
        out_shape=pltpu.VMEM((token_count, width), bf16),
        in_specs=[hbm] * 15,
        out_specs=vmem,
        scratch_shapes=[
            pltpu.VMEM((n_sp, experts, cap, width), bf16),
            pltpu.VMEM((token_count, width), jnp.float32),
            pltpu.VMEM((n_sp, experts, cap, width), bf16),
            pltpu.VMEM((n_sp // 2, n_tp // 2 - 1, experts, cap, width), bf16),
            pltpu.VMEM((token_count, width * n_tp), bf16),
            pltpu.VMEM((token_count, width), bf16),
            pltpu.VMEM((channels, token_count), bf16),
            pltpu.VMEM((channels, edge), bf16),
            pltpu.VMEM((channels, edge), bf16),
            pltpu.VMEM((channels * n_tp, token_count), bf16),
            pltpu.VMEM((n_tp, channels, edge), bf16),
            pltpu.VMEM((channels * n_tp, token_count), bf16),
            pltpu.VMEM((n_tp, 8, token_count), jnp.float32),
            pltpu.VMEM((n_tp, 8, width), jnp.float32),
            pltpu.VMEM((8, width * n_tp), jnp.float32),
            pltpu.VMEM((n_sp, 8, lanes), jnp.float32),
            pltpu.VMEM((n_sp, 8, lanes), jnp.float32),
            pltpu.VMEM((8, token_count), jnp.float32),
            pltpu.VMEM((8, token_count), jnp.float32),
            pltpu.VMEM((routes.shape[1], token_count), jnp.int32),
            pltpu.VMEM((token_count, width), bf16),
            pltpu.VMEM((experts, n_sp * cap, width * n_tp), bf16),
            pltpu.VMEM((experts, n_sp * cap, hidden_width * n_tp), bf16),
            pltpu.VMEM((token_count, width * n_tp), bf16),
            pltpu.VMEM((n_tp, token_count, shared_gate.shape[1]), bf16),
            pltpu.VMEM((n_sp, experts, cap, width), bf16),
            pltpu.VMEM(outer_gate.shape, bf16),
            pltpu.VMEM(inner_gate.shape, bf16),
            pltpu.VMEM(conv_input.shape, bf16),
            pltpu.VMEM(conv_taps.shape, bf16),
            pltpu.VMEM(norm_gain.shape, bf16),
            pltpu.VMEM(routes.shape[::-1], jnp.int32),
            pltpu.VMEM(route_scores.shape[::-1], jnp.float32),
            pltpu.VMEM(mix_weight.shape, bf16),
            pltpu.VMEM(residual.shape, bf16),
            pltpu.VMEM(expert_gate.shape, bf16),
            pltpu.VMEM(expert_up.shape, bf16),
            pltpu.VMEM(expert_down.shape, bf16),
            pltpu.VMEM(shared_gate.shape, bf16),
            pltpu.VMEM(shared_up.shape, bf16),
            pltpu.VMEM(shared_down.shape, bf16),
            dma((15,)),
            dma((2,)),
            dma((2,)),
            dma((n_sp,)),
            dma((n_sp,)),
            dma((n_sp // 2, n_tp // 2)),
            dma((n_sp // 2, n_tp // 2)),
            dma((n_sp,)),
            dma((n_sp,)),
            dma((3,)),
            dma((3,)),
            dma((slots,)),
            dma((slots,)),
            dma((slots,)),
            dma((slots,)),
            dma((slots,)),
            dma((slots,)),
            dma((n_sp, experts)),
            dma((n_sp, experts)),
        ],
        compiler_params=pltpu.CompilerParams(
            collective_id=0, has_side_effects=True, vmem_limit_bytes=VMEM_LIMIT
        ),
    )(
        outer_gate,
        inner_gate,
        conv_input,
        conv_taps,
        norm_gain,
        routes.T,
        route_scores.T,
        mix_weight,
        residual,
        expert_gate,
        expert_up,
        expert_down,
        shared_gate,
        shared_up,
        shared_down,
    )


def solution(mesh):
    in_specs = (
        P("tp", "sp"),
        P("tp", "sp"),
        P("tp", "sp"),
        P(None, "tp"),
        P(None, "tp"),
        P("sp", "tp"),
        P("tp"),
        P("sp", None),
        P("sp", None),
        P("sp", None, "tp"),
        P("sp", None, "tp"),
        P("sp", None, "tp"),
        P(None, "tp"),
        P(None, "tp"),
        P(None, "tp"),
    )
    out_specs = P("sp", "tp")
    return jax.shard_map(local, mesh=mesh, in_specs=in_specs, out_specs=out_specs, check_vma=False)
```
